32 devices in a mesh: fs: 8 (over z, y), tp: 4 (over x, core).
Axes of the slice: x: 2, y: 2, z: 4, core: 2. Of those that a mesh axis runs over, the one named last changes fastest.
Arguments:
- tokens: bfloat16 [6144, 2048], P('fs', 'tp'), may hold values from -40 to 40
- gain_one: float32 [2048], P('tp'), may hold values from 0.1 to 1.9
- w_gate: float32 [2048, 3072], P('fs', 'tp'), may hold values from -0.125 to 0.125
- w_up: float32 [2048, 3072], P('fs', 'tp'), may hold values from -0.125 to 0.125
- w_down: float32 [3072, 2048], P('tp', 'fs'), may hold values from -0.109375 to 0.109375
- scale_gate: float32 [3072], P('tp'), may hold values from 0.5 to 2
- scale_up: float32 [3072], P('tp'), may hold values from 0.5 to 2
- scale_down: float32 [2048], P('tp'), may hold values from 0.5 to 2
- gain_mix: float32 [2048], P('tp'), may hold values from 0.1 to 1.9
- w_query: float32 [2048, 2048], P('fs', 'tp'), may hold values from -0.125 to 0.125
- w_key: float32 [2048, 2048], P('fs', 'tp'), may hold values from -0.125 to 0.125
- w_value: float32 [2048, 2048], P('fs', 'tp'), may hold values from -0.125 to 0.125
- w_outgate: float32 [2048, 2048], P('fs', 'tp'), may hold values from -0.125 to 0.125
- scale_query: float32 [2048], P('tp'), may hold values from 0.5 to 2
- scale_key: float32 [2048], P('tp'), may hold values from 0.5 to 2
- scale_value: float32 [2048], P('tp'), may hold values from 0.5 to 2
- scale_outgate: float32 [2048], P('tp'), may hold values from 0.5 to 2
- ret_gain: float32 [2048], P('tp'), may hold values from 0.1 to 1.9
- decay_rate: float32 [8], P('tp'), may hold values from 0 to 2
- w_mix: float32 [2048, 2048], P('tp', 'fs'), may hold values from -0.125 to 0.125
- scale_mix: float32 [2048], P('tp'), may hold values from 0.5 to 2
- gain_two: float32 [2048], P('tp'), may hold values from 0.1 to 1.9
Outputs:
- layer_out: bfloat16 [6144, 2048], P('fs', 'tp')
The draws below stay inside these ranges and needn't reach their ends.
All inputs are finite; a program needn't handle non-finite values.
Results may differ from the reference program's by a relative error of at most 0.022.
Values may be sent and summed in bfloat16 or wider, within the bound.
A program may use at most 128 MiB of HBM per device.

```python
import math
import jax
import jax.numpy as jnp
from jax import lax

D = 2048
FF = 3072
HEADS = 8
LEN = 256
BLK = 128
RW = 2048
TOKENS = 6144
N_TP = 4


def draw_tokens(key, part):
    base = jax.random.normal(jax.random.fold_in(key, 13), (TOKENS, D), jnp.float32)
    logs = jax.random.uniform(jax.random.fold_in(key, 14), (TOKENS, 8), jnp.float32, -1.2, 1.2)
    factors = jnp.repeat(jnp.exp(logs), D // 8, axis=1)
    return (base * factors).astype(jnp.bfloat16)


def draw_decay_rate(key, part):
    picks = jax.random.randint(jax.random.fold_in(key, 21), (HEADS,), 0, 2)
    quick = jax.random.uniform(jax.random.fold_in(key, 22), (HEADS,), jnp.float32, 4.0 / BLK, 16.0 / BLK)
    slower = jax.random.uniform(jax.random.fold_in(key, 23), (HEADS,), jnp.float32, 0.3 / LEN, 2.3 / LEN)
    return jnp.where(picks == 1, quick, slower)


def steps_of(rng, extent, split, low, high):
    factor_of, own = 1.0, jax.random.fold_in(rng, 6)
    for position, blocks in split:
        heights = jnp.exp(jax.random.uniform(jax.random.fold_in(own, position), (blocks,), jnp.float32, low / len(split), high / len(split)))
        factor_of = factor_of * jnp.repeat(heights, extent[position] // blocks).reshape([-1 if axis == position else 1 for axis in range(len(extent))])
    return factor_of


def centred(rng, dims, deviation, most, split=(), held_as=jnp.bfloat16):
    array = deviation * jax.random.normal(rng, dims, jnp.float32)
    if split:
        array = array * steps_of(rng, dims, split, -0.22, 0.18)
    return jnp.clip(array, -most, most).astype(held_as)


def setup_inputs(seed: int = 0) -> dict:
    seeds = jax.random.split(jax.random.key(seed), 23)
    tokens = draw_tokens(jax.random.fold_in(seeds[22], 71), 0)
    gain_one = jnp.clip(1.0 + 0.18 * jax.random.normal(seeds[1], (D,), jnp.float32), 0.1, 1.9)
    w_gate = centred(seeds[2], (D, FF), D ** -0.5, 0.125, ((0, 8), (1, 4)), jnp.float32)
    w_up = centred(seeds[3], (D, FF), D ** -0.5, 0.125, ((0, 8), (1, 4)), jnp.float32)
    w_down = centred(seeds[4], (FF, D), FF ** -0.5, 0.109375, ((0, 4), (1, 8)), jnp.float32)
    scale_gate = jnp.clip(jnp.exp(math.log(2.0) - 1.3862944 * jax.random.uniform(seeds[5], (FF,), jnp.float32) ** steps_of(seeds[5], (FF,), ((0, 4),), -0.2, 0.2)), 0.5, 2.0)
    scale_up = jnp.clip(jnp.exp(math.log(2.0) - 1.3862944 * jax.random.uniform(seeds[6], (FF,), jnp.float32) ** steps_of(seeds[6], (FF,), ((0, 4),), -0.2, 0.2)), 0.5, 2.0)
    scale_down = jnp.clip(jnp.exp(math.log(2.0) - 1.3862944 * jax.random.uniform(seeds[7], (D,), jnp.float32) ** steps_of(seeds[7], (D,), ((0, 4),), -0.2, 0.2)), 0.5, 2.0)
    gain_mix = jnp.clip(1.0 + 0.18 * jax.random.normal(seeds[8], (D,), jnp.float32), 0.1, 1.9)
    w_query = centred(seeds[9], (D, RW), D ** -0.5, 0.125, ((0, 8), (1, 4)), jnp.float32)
    w_key = centred(seeds[10], (D, RW), D ** -0.5, 0.125, ((0, 8), (1, 4)), jnp.float32)
    w_value = centred(seeds[11], (D, RW), D ** -0.5, 0.125, ((0, 8), (1, 4)), jnp.float32)
    w_outgate = centred(seeds[12], (D, RW), D ** -0.5, 0.125, ((0, 8), (1, 4)), jnp.float32)
    scale_query = jnp.clip(jnp.exp(math.log(2.0) - 1.3862944 * jax.random.uniform(seeds[13], (RW,), jnp.float32) ** steps_of(seeds[13], (RW,), ((0, 4),), -0.2, 0.2)), 0.5, 2.0)
    scale_key = jnp.clip(jnp.exp(math.log(2.0) - 1.3862944 * jax.random.uniform(seeds[14], (RW,), jnp.float32) ** steps_of(seeds[14], (RW,), ((0, 4),), -0.2, 0.2)), 0.5, 2.0)
    scale_value = jnp.clip(jnp.exp(math.log(2.0) - 1.3862944 * jax.random.uniform(seeds[15], (RW,), jnp.float32) ** steps_of(seeds[15], (RW,), ((0, 4),), -0.2, 0.2)), 0.5, 2.0)
    scale_outgate = jnp.clip(jnp.exp(math.log(2.0) - 1.3862944 * jax.random.uniform(seeds[16], (RW,), jnp.float32) ** steps_of(seeds[16], (RW,), ((0, 4),), -0.2, 0.2)), 0.5, 2.0)
    ret_gain = jnp.clip(1.0 + 0.18 * jax.random.normal(seeds[17], (RW,), jnp.float32), 0.1, 1.9)
    decay_rate = draw_decay_rate(jax.random.fold_in(seeds[22], 71), 0)
    w_mix = centred(seeds[19], (RW, D), RW ** -0.5, 0.125, ((0, 4), (1, 8)), jnp.float32)
    scale_mix = jnp.clip(jnp.exp(math.log(2.0) - 1.3862944 * jax.random.uniform(seeds[20], (D,), jnp.float32) ** steps_of(seeds[20], (D,), ((0, 4),), -0.2, 0.2)), 0.5, 2.0)
    gain_two = jnp.clip(1.0 + 0.18 * jax.random.normal(seeds[21], (D,), jnp.float32), 0.1, 1.9)
    return dict(tokens=tokens, gain_one=gain_one, w_gate=w_gate, w_up=w_up, w_down=w_down, scale_gate=scale_gate, scale_up=scale_up, scale_down=scale_down, gain_mix=gain_mix, w_query=w_query, w_key=w_key, w_value=w_value, w_outgate=w_outgate, scale_query=scale_query, scale_key=scale_key, scale_value=scale_value, scale_outgate=scale_outgate, ret_gain=ret_gain, decay_rate=decay_rate, w_mix=w_mix, scale_mix=scale_mix, gain_two=gain_two)


EPS = 1e-06
HEAD_EPS = 0.1

def rms_rows(hidden_in, norm_gain):
    widened = hidden_in.astype(jnp.float32)
    scaled = widened * lax.rsqrt(lax.optimization_barrier(jnp.mean(widened * widened, axis=1, keepdims=True)) + EPS) * norm_gain
    return scaled.astype(jnp.bfloat16)

def project(features, weight, column_scale):
    return jnp.dot(features, weight.astype(jnp.bfloat16), preferred_element_type=jnp.float32) * column_scale

def split_sum(left, weight, parts):
    width = left.shape[1] // parts

    def add_block(index, total):
        start = (index * width).astype(jnp.int32)
        columns = lax.dynamic_slice_in_dim(left, start, width, 1)
        block = lax.dynamic_slice_in_dim(weight, start, width, 0).astype(jnp.bfloat16)
        partial_value = jnp.dot(columns, block, preferred_element_type=jnp.float32).astype(jnp.bfloat16)
        partial_value = lax.optimization_barrier(partial_value)
        return total + partial_value.astype(jnp.float32)
    return lax.fori_loop(0, parts, add_block, jnp.zeros((left.shape[0], weight.shape[1]), jnp.float32))

def feed_forward(features, w_gate, w_up, w_down, scale_gate, scale_up, scale_down):
    gate_pre = project(features, w_gate, scale_gate)
    up_pre = project(features, w_up, scale_up)
    hidden = (jax.nn.silu(gate_pre) * up_pre).astype(jnp.bfloat16)
    return split_sum(hidden, w_down, N_TP) * scale_down

def rotate_pairs(values):
    paired = values.reshape(values.shape[:-1] + (values.shape[-1] // 2, 2))
    return jnp.stack((-paired[..., 1], paired[..., 0]), axis=-1).reshape(values.shape)

def retain(query_rows, key_rows, value_rows, decay_rate, length, block):
    highest = lax.Precision.HIGHEST
    total_rows = query_rows.shape[0]
    heads = decay_rate.shape[0]
    head_size = query_rows.shape[1] // heads
    sequences = total_rows // length
    nblocks = length // block

    def split_heads(values):
        return values.astype(jnp.float32).reshape(sequences, length, heads, head_size)
    freq = 1.0 / 10000.0 ** jnp.linspace(0.0, 1.0, head_size // 2, dtype=jnp.float32)
    freq = jnp.repeat(freq, 2)
    angles = jnp.arange(length, dtype=jnp.float32)[:, None] * freq[None, :]
    sines = jnp.sin(angles)[None, :, None, :]
    cosines = jnp.cos(angles)[None, :, None, :]
    queries = split_heads(query_rows)
    queries = queries * cosines + rotate_pairs(queries) * sines
    keys_all = split_heads(key_rows) * head_size ** (-0.5)
    keys_all = keys_all * cosines + rotate_pairs(keys_all) * sines
    values_all = split_heads(value_rows)
    log_decay = -decay_rate.astype(jnp.float32)
    offsets = jnp.arange(block, dtype=jnp.float32)
    distance = offsets[:, None] - offsets[None, :]
    inside = jnp.where(distance >= 0, jnp.exp(log_decay[:, None, None] * jnp.maximum(distance, 0.0)), 0.0)
    query_decay = jnp.exp(log_decay[None, :] * (offsets[:, None] + 1.0))
    key_decay = jnp.exp(log_decay[None, :] * (block - 1.0 - offsets[:, None]))
    block_decay = jnp.exp(log_decay * block)

    def to_blocks(values):
        return jnp.moveaxis(values.reshape(sequences, nblocks, block, heads, head_size), 1, 0)

    def advance(carried, pieces):
        query_blk, key_blk, value_blk = pieces
        scores = jnp.einsum('snhd,smhd->shnm', query_blk, key_blk, precision=highest) * inside
        within = jnp.einsum('shnm,smhe->snhe', scores, value_blk, precision=highest)
        across = jnp.einsum('snhd,shde->snhe', query_blk, carried, precision=highest) * query_decay[None, :, :, None]
        weighted = key_blk * key_decay[None, :, :, None]
        carried = carried * block_decay[None, :, None, None] + jnp.einsum('smhd,smhe->shde', weighted, value_blk, precision=highest)
        return (carried, within + across)
    initial = jnp.zeros((sequences, heads, head_size, head_size), jnp.float32)
    _, results = lax.scan(advance, initial, (to_blocks(queries), to_blocks(keys_all), to_blocks(values_all)))
    results = jnp.moveaxis(results, 0, 1).reshape(sequences, length, heads, head_size)
    results = results * lax.rsqrt(lax.optimization_barrier(jnp.mean(results * results, axis=-1, keepdims=True)) + HEAD_EPS)
    return results.reshape(total_rows, heads * head_size)

def reference(tokens, gain_one, w_gate, w_up, w_down, scale_gate, scale_up, scale_down, gain_mix, w_query, w_key, w_value, w_outgate, scale_query, scale_key, scale_value, scale_outgate, ret_gain, decay_rate, w_mix, scale_mix, gain_two):
    ffn_one = feed_forward(rms_rows(tokens, gain_one), w_gate, w_up, w_down, scale_gate, scale_up, scale_down)
    first = (tokens.astype(jnp.float32) + 0.5 * ffn_one).astype(jnp.bfloat16)
    features = rms_rows(first, gain_mix)
    query_rows = project(features, w_query, scale_query).astype(jnp.bfloat16)
    key_rows = project(features, w_key, scale_key).astype(jnp.bfloat16)
    value_rows = project(features, w_value, scale_value).astype(jnp.bfloat16)
    outgate_rows = project(features, w_outgate, scale_outgate).astype(jnp.bfloat16)
    retained = retain(query_rows, key_rows, value_rows, decay_rate, LEN, BLK)
    mixed = (retained * ret_gain * jax.nn.silu(outgate_rows.astype(jnp.float32))).astype(jnp.bfloat16)
    second = (first.astype(jnp.float32) + split_sum(mixed, w_mix, N_TP) * scale_mix).astype(jnp.bfloat16)
    ffn_two = feed_forward(rms_rows(second, gain_two), w_gate, w_up, w_down, scale_gate, scale_up, scale_down)
    return (second.astype(jnp.float32) + 0.5 * ffn_two).astype(jnp.bfloat16)
```

```python
import functools
from types import SimpleNamespace

import jax
import jax.numpy as jnp
import numpy as np
from jax import lax
from jax.experimental import pallas as pl
from jax.experimental.pallas import tpu as pltpu
from jax.sharding import PartitionSpec as P

LEN = 256
EPS = 1e-06
HEAD_EPS = 0.1
MESH = pl.DeviceIdType.MESH
BF16 = jnp.bfloat16
F32 = jnp.float32
WEIGHTS = ("gate", "up", "down", "query", "key", "value", "outgate", "mix")
DIMS = (0, 0, 1, 0, 0, 0, 0, 1)
PARTS = (2, 2, 2, 1, 1, 1, 1, 2)
ALONG_Z = ((0, 0), (3, 0))


def cols_at(index, width):
    return pl.ds(pl.multiple_of(index * width, width), width)


def remote(src, dst, send_sem, recv_sem, axis, target):
    return pltpu.make_async_remote_copy(
        src_ref=src,
        dst_ref=dst,
        send_sem=send_sem,
        recv_sem=recv_sem,
        device_id={axis: target},
        device_id_type=MESH,
    )


def dot(left, right):
    return jnp.dot(left, right, preferred_element_type=F32)


class TpGroup:
    def __init__(self, ntp):
        self.ntp, self.nx = ntp, ntp // 2
        self.t = lax.axis_index("tp")
        self.core, self.chip = lax.rem(self.t, 2), lax.div(self.t, 2)
        self.partner = self.chip * 2 + (1 - self.core)

    def along_x(self, offset, core):
        return lax.rem(self.chip + offset, self.nx) * 2 + core

    def greet(self, barrier):
        for offset in range(1, self.ntp):
            target = lax.rem(self.t + offset, self.ntp)
            pl.semaphore_signal(barrier, inc=1, device_id={"tp": target}, device_id_type=MESH)
        return self.ntp - 1


class TpGather:
    def __init__(self, group, src, out, sems, rows):
        self.group = group
        self.src, self.out, self.rows = src, out, rows
        self.sends, self.forwards, self.recvs = sems
        self.width = src.shape[1]

    def at(self, piece):
        return pl.ds(piece * self.rows, self.rows)

    def place(self, index, piece):
        return self.out.at[self.at(piece), cols_at(index, self.width)]

    def own_sends(self, piece):
        group = self.group
        copies = []
        for offset in range(group.nx - 1, -1, -1):
            target = group.along_x(offset, group.core) if offset else group.partner
            copies.append(
                remote(
                    self.src.at[self.at(piece)], self.place(group.t, piece),
                    self.sends.at[offset, piece], self.recvs.at[group.t, piece], "tp", target,
                )
            )
        return copies

    def forward(self, offset, piece):
        group = self.group
        index = group.along_x(group.nx - offset, group.core)
        block = self.place(index, piece)
        return remote(
            block, block, self.forwards.at[offset, piece], self.recvs.at[index, piece],
            "tp", group.partner,
        )

    def arrived(self, index, piece):
        block = self.place(index, piece)
        remote(
            block, block, self.sends.at[0, piece], self.recvs.at[index, piece],
            "tp", self.group.partner,
        ).wait_recv()

    def start(self, piece):
        for copy in self.own_sends(piece):
            copy.start()

    def relay(self, piece):
        group = self.group
        for offset in range(1, group.nx):
            self.arrived(group.along_x(group.nx - offset, group.core), piece)
            self.forward(offset, piece).start()

    def complete(self, piece):
        group = self.group
        for offset in range(group.nx):
            self.arrived(group.along_x(offset, 1 - group.core), piece)
        for offset in range(1, group.nx):
            self.forward(offset, piece).wait_send()

    def finish(self, piece):
        for copy in self.own_sends(piece):
            copy.wait_send()


class TpReduce:
    def __init__(self, group, part, pair, one, two, sems, rows, width):
        self.group, self.part, self.pair, self.one, self.two = group, part, pair, one, two
        self.s1, self.v1, self.s2, self.v2 = sems
        self.rows, self.width = rows, width

    def at(self, piece):
        return pl.ds(piece * self.rows, self.rows)

    def block(self, offset, core):
        return cols_at(self.group.along_x(offset, core), self.width)

    def to_partner(self, offset, piece):
        return remote(
            self.part.at[self.at(piece), self.block(offset, 1 - self.group.core)],
            self.one.at[offset, self.at(piece)],
            self.s1.at[offset, piece], self.v1.at[offset, piece], "tp", self.group.partner,
        )

    def across(self, offset, piece):
        return remote(
            self.pair.at[offset - 1, self.at(piece)],
            self.two.at[offset - 1, self.at(piece)],
            self.s2.at[offset - 1, piece], self.v2.at[offset - 1, piece],
            "tp", self.group.along_x(offset, self.group.core),
        )

    def start(self, piece):
        for offset in range(self.group.nx - 1, -1, -1):
            self.to_partner(offset, piece).start()

    def cross(self, piece):
        at = self.at(piece)
        for offset in range(self.group.nx - 1, 0, -1):
            self.to_partner(offset, piece).wait_recv()
            mine = self.part[at, self.block(offset, self.group.core)].astype(F32)
            self.pair[offset - 1, at] = (mine + self.one[offset, at].astype(F32)).astype(BF16)
            self.across(offset, piece).start()

    def total(self, piece):
        at = self.at(piece)
        self.to_partner(0, piece).wait_recv()
        value = self.part[at, self.block(0, self.group.core)].astype(F32)
        value = value + self.one[0, at].astype(F32)
        for offset in range(1, self.group.nx):
            self.across(offset, piece).wait_recv()
            value = value + self.two[offset - 1, at].astype(F32)
        return value

    def finish(self, piece):
        for offset in range(self.group.nx):
            self.to_partner(offset, piece).wait_send()
        for offset in range(1, self.group.nx):
            self.across(offset, piece).wait_send()


class FsStream:
    def __init__(self, nfs, ny, pieces, sends, recvs):
        self.ny, self.nz = ny, nfs // ny
        self.f = lax.axis_index("fs")
        self.z, self.y = lax.div(self.f, ny), lax.rem(self.f, ny)
        self.pieces = pieces
        self.sends, self.recvs = sends, recvs
        self.events, self.done = self.schedule(), 0

    def whole_z(self, p):
        return self.pieces[p].along_z

    def place(self, p, index):
        piece = self.pieces[p]
        if piece.dim == 0:
            start = pl.multiple_of(index * piece.rows + piece.start, 16)
            return piece.buf.at[pl.ds(start, piece.size)]
        return piece.buf.at[pl.ds(piece.start, piece.size), cols_at(index, piece.cols)]

    def move(self, p, kind, index, target):
        block = self.place(p, index)
        return remote(
            block, block, self.sends.at[kind, index, p], self.recvs.at[index, p], "fs", target
        )

    def arrived(self, p, index):
        self.move(p, 0, index, self.f).wait_recv()

    def move_z(self, p, step, index, act):
        inside = (self.z < self.nz - 1) if step > 0 else (self.z > 0)

        @pl.when(inside)
        def _():
            act(self.move(p, 0 if step > 0 else 1, index, self.f + step * self.ny))

    def move_y(self, p, index, act):
        for offset in range(1, self.ny):
            target = self.z * self.ny + lax.rem(self.y + offset, self.ny)
            act(self.move(p, 1 + offset, index, target))

    def others(self, zs):
        return [zs * self.ny + lax.rem(self.y + offset, self.ny) for offset in range(1, self.ny)]

    def own(self, p, act, wait):
        self.move_y(p, self.f, act)
        for step in (1, -1):
            self.move_z(p, step, self.f, act)

    def side(self, p, act, wait):
        for index in self.others(self.z):
            if wait:
                self.arrived(p, index)
            for step in (1, -1):
                self.move_z(p, step, index, act)

    def relay(self, distance, p, act, wait):
        for step in (1, -1):
            zs = self.z - step * distance

            @pl.when(jnp.logical_and(zs >= 0, zs < self.nz))
            def _():
                same = zs * self.ny + self.y
                for index in [same] + (self.others(zs) if self.whole_z(p) else []):
                    if wait:
                        self.arrived(p, index)
                    self.move_z(p, step, index, act)
                    if not self.whole_z(p):
                        self.move_y(p, index, act)

    def schedule(self):
        count = len(self.pieces)
        events = [(-1, functools.partial(self.own, 0))]
        for tick in range(count + self.nz - 2):
            if tick + 1 < count:
                events.append((tick, functools.partial(self.own, tick + 1)))
            if tick < count and self.whole_z(tick):
                events.append((tick, functools.partial(self.side, tick)))
            for distance in range(1, self.nz):
                if 0 <= tick + 1 - distance < count:
                    events.append((tick, functools.partial(self.relay, distance, tick + 1 - distance)))
        return events

    def some(self, count):
        for _, event in self.events[self.done : self.done + count]:
            event(lambda copy: copy.start(), True)
        self.done = min(self.done + count, len(self.events))

    def upto(self, tick):
        ahead = sum(1 for at, _ in self.events[self.done :] if at <= tick)
        self.some(ahead)

    def need(self, p):
        self.upto(p + self.nz - 2)
        if not self.whole_z(p):
            for zs in range(self.nz):
                for index in self.others(zs):
                    self.arrived(p, index)

    def finish(self):
        for _, event in self.events:
            event(lambda copy: copy.wait_send(), False)

    def greet(self, barrier):
        ny, z, f = self.ny, self.z, self.f
        for index in self.others(z):
            pl.semaphore_signal(barrier, inc=1, device_id={"fs": index}, device_id_type=MESH)

        @pl.when(z > 0)
        def _():
            pl.semaphore_signal(barrier, inc=1, device_id={"fs": f - ny}, device_id_type=MESH)

        @pl.when(z < self.nz - 1)
        def _():
            pl.semaphore_signal(barrier, inc=1, device_id={"fs": f + ny}, device_id_type=MESH)

        ends = (z > 0).astype(jnp.int32) + (z < self.nz - 1).astype(jnp.int32)
        return ends + (ny - 1)


def layer_kernel(nfs, ntp, ny, names, *refs):
    r = SimpleNamespace(**dict(zip(names, refs)))
    rows, width = r.tok.shape
    count = rows // LEN
    chunks = range(count)
    group = TpGroup(ntp)
    shards = [getattr(r, "w_" + name) for name in WEIGHTS]
    wholes = [getattr(r, name) for name in WEIGHTS]
    pieces, first_of = [], {}
    for i, name in enumerate(WEIGHTS):
        first_of[name] = len(pieces)
        size = shards[i].shape[0] // PARTS[i]
        for part in range(PARTS[i]):
            pieces.append(
                SimpleNamespace(
                    buf=wholes[i], dim=DIMS[i], rows=shards[i].shape[0], cols=shards[i].shape[1],
                    start=part * size, size=size, along_z=(i, part) in ALONG_Z,
                )
            )
    stream = FsStream(nfs, ny, pieces, r.w_send, r.w_recv)

    def need(name):
        i = WEIGHTS.index(name)
        for part in range(PARTS[i]):
            stream.need(first_of[name] + part)

    def at(c):
        return pl.ds(c * LEN, LEN)

    barrier = pltpu.get_barrier_semaphore()
    greeted = group.greet(barrier) + stream.greet(barrier)
    loads = [
        pltpu.make_async_copy(shards[i], getattr(r, "stage_" + name), r.load_sem.at[i])
        for i, name in enumerate(WEIGHTS)
    ]
    for load in loads:
        load.start()

    def cast(i):
        loads[i].wait()
        shard = shards[i].shape
        value = getattr(r, "stage_" + WEIGHTS[i])[...].astype(BF16)
        if DIMS[i] == 0:
            wholes[i][pl.ds(pl.multiple_of(stream.f * shard[0], shard[0]), shard[0]), :] = value
        else:
            wholes[i][:, cols_at(stream.f, shard[1])] = value

    r.gain_own[...] = jnp.zeros(r.gain_own.shape, F32)
    for row, ref in enumerate((r.gain_one, r.gain_mix, r.gain_two)):
        r.gain_own[row : row + 1, :] = ref[...]
    cast(0)
    cast(1)
    r.full_0[:, cols_at(group.t, width)] = r.tok[...]
    r.gains[:, cols_at(group.t, width)] = r.gain_own[...]
    pl.semaphore_wait(barrier, greeted)

    gain_gather = TpGather(group, r.gain_own, r.gains, (r.n_send, r.n_fwd, r.n_recv), 8)
    gathers = [
        TpGather(group, src, full, (r.g_send.at[i], r.g_fwd.at[i], r.g_recv.at[i]), LEN)
        for i, (src, full) in enumerate(
            ((r.tok, r.full_0), (r.first, r.full_1), (r.second, r.full_2))
        )
    ]
    reduces = [
        TpReduce(
            group, r.part, r.pair, r.one.at[i], r.two.at[i],
            (r.r_s1.at[i], r.r_v1.at[i], r.r_s2.at[i], r.r_v2.at[i]), LEN, width,
        )
        for i in range(3)
    ]
    gain_gather.start(0)
    for c in chunks:
        gathers[0].start(c)
    stream.some(2)
    for i in range(2, len(WEIGHTS)):
        cast(i)

    def norm(full, row, c):
        gain = r.gains[row : row + 1, :]
        step = 32

        def body(i, carry):
            some = pl.ds(pl.multiple_of(c * LEN + i * step, step), step)
            v = full[some, :].astype(F32)
            mean = jnp.mean(v * v, axis=1, keepdims=True)
            full[some, :] = (v * lax.rsqrt(mean + EPS) * gain).astype(BF16)
            return carry

        lax.fori_loop(0, LEN // step, body, 0)

    def gate_up(full, c):
        units = r.gate.shape[1]
        tile = 256 if units % 256 == 0 else 128

        def body(n, carry):
            cols = cols_at(n, tile)
            x = full[at(c), :]
            g = dot(x, r.gate[:, cols]) * r.scale_gate[:, cols]
            u = dot(x, r.up[:, cols]) * r.scale_up[:, cols]
            r.hidden[at(c), cols] = (g / (1.0 + jnp.exp(-g)) * u).astype(BF16)
            return carry

        lax.fori_loop(0, units // tile, body, 0)

    def partial(left, weight, c):
        def body(n, carry):
            cols = cols_at(n, width)
            r.part[at(c), cols] = dot(left[at(c), :], weight[:, cols]).astype(BF16)
            return carry

        lax.fori_loop(0, ntp, body, 0)

    def project(name, full):
        weight, scale, out = getattr(r, name), getattr(r, "scale_" + name), getattr(r, "a_" + name)

        def body(c, carry):
            some = pl.ds(pl.multiple_of(c * LEN, LEN), LEN)
            out[some, :] = (dot(full[some, :], weight[...]) * scale[...]).astype(BF16)
            return carry

        lax.fori_loop(0, count, body, 0)

    def retain():
        heads = r.rate.shape[1]
        size = width // heads
        even = lax.rem(lax.broadcasted_iota(jnp.int32, (LEN, size), 1), 2) == 0
        distance = lax.broadcasted_iota(jnp.int32, (LEN, LEN), 0) - lax.broadcasted_iota(
            jnp.int32, (LEN, LEN), 1
        )

        def body(i, carry):
            c, h = lax.div(i, heads), lax.rem(i, heads)
            some, cols = pl.ds(pl.multiple_of(c * LEN, LEN), LEN), cols_at(h, size)

            def turned(ref):
                v = ref[some, cols].astype(F32)
                swapped = jnp.where(even, -pltpu.roll(v, size - 1, 1), pltpu.roll(v, 1, 1))
                return v * r.cosines[...] + swapped * r.sines[...]

            q = turned(r.a_query).astype(BF16)
            k = (turned(r.a_key) * size ** -0.5).astype(BF16)
            scores = lax.dot_general(q, k, (((1,), (1,)), ((), ())), preferred_element_type=F32)
            decay = jnp.exp(-r.rate[0, h] * jnp.maximum(distance, 0).astype(F32))
            scores = jnp.where(distance >= 0, scores * decay, 0.0).astype(BF16)
            kept = dot(scores, r.a_value[some, cols])
            kept = kept * lax.rsqrt(jnp.mean(kept * kept, axis=1, keepdims=True) + HEAD_EPS)
            g = r.a_outgate[some, cols].astype(F32)
            gated = kept * r.ret_gain[:, cols] * (g / (1.0 + jnp.exp(-g)))
            r.mixed[some, cols] = gated.astype(BF16)
            return carry

        lax.fori_loop(0, count * heads, body, 0)

    def settle(i, c, factor, scale, res, out):
        value = res[at(c), :].astype(F32) + factor * reduces[i].total(c) * scale[...]
        value = value.astype(BF16)
        out[at(c), :] = value
        if i < 2:
            full = (r.full_1, r.full_2)[i]
            full[at(c), cols_at(group.t, width)] = value
            gathers[i + 1].start(c)

    gain_gather.relay(0)
    for c in chunks:
        stream.upto(c)
        gathers[0].relay(c)
    gain_gather.complete(0)
    for c in chunks:
        stream.some(1)
        gathers[0].complete(c)
        norm(r.full_0, 0, c)
    need("gate")
    need("up")
    for c in chunks:
        gate_up(r.full_0, c)
        stream.some(1)
    need("down")
    for c in chunks:
        partial(r.hidden, r.down, c)
        reduces[0].start(c)
        stream.some(1)
    for c in chunks:
        reduces[0].cross(c)
        stream.some(1)
    for c in chunks:
        settle(0, c, 0.5, r.scale_down, r.tok, r.first)
        stream.some(1)
    for c in chunks:
        gathers[1].relay(c)
        stream.some(1)
    for c in chunks:
        gathers[1].complete(c)
        norm(r.full_1, 1, c)
        reduces[0].finish(c)
    for name in ("query", "key", "value", "outgate"):
        need(name)
        project(name, r.full_1)
        stream.some(1)
    retain()
    need("mix")
    for c in chunks:
        partial(r.mixed, r.mix, c)
        reduces[1].start(c)
    for c in chunks:
        reduces[1].cross(c)
    for c in chunks:
        settle(1, c, 1.0, r.scale_mix, r.first, r.second)
    gathers[2].relay(0)
    for c in chunks:
        gathers[2].complete(c)
        norm(r.full_2, 2, c)
        if c > 0:
            reduces[2].cross(c - 1)
        gate_up(r.full_2, c)
        if c + 1 < count:
            gathers[2].relay(c + 1)
        reduces[1].finish(c)
        partial(r.hidden, r.down, c)
        reduces[2].start(c)
    reduces[2].cross(count - 1)
    for c in chunks:
        settle(2, c, 0.5, r.scale_down, r.second, r.out)
    for c in chunks:
        reduces[2].finish(c)
        for gather in gathers:
            gather.finish(c)
    gain_gather.finish(0)
    stream.finish()


def vmem():
    return pl.BlockSpec(memory_space=pltpu.VMEM)


def dma(*shape):
    return pltpu.SemaphoreType.DMA(shape)


def along_y_of(nfs, ntp):
    return ntp // 2 if nfs % (ntp // 2) == 0 else 1


def tables(length, width):
    freq = np.float32(1.0) / np.float32(10000.0) ** np.linspace(0.0, 1.0, width // 2, dtype=np.float32)
    angles = np.arange(length, dtype=np.float32)[:, None] * np.repeat(freq, 2)[None, :]
    return jnp.asarray(np.cos(angles)), jnp.asarray(np.sin(angles))


def per_device(
    nfs, ntp,
    tokens, gain_one, w_gate, w_up, w_down, scale_gate, scale_up, scale_down,
    gain_mix, w_query, w_key, w_value, w_outgate,
    scale_query, scale_key, scale_value, scale_outgate,
    ret_gain, decay_rate, w_mix, scale_mix, gain_two,
):
    ny, nx = along_y_of(nfs, ntp), ntp // 2
    rows, width = tokens.shape
    count = rows // LEN
    model = width * ntp
    weights = (w_gate, w_up, w_down, w_query, w_key, w_value, w_outgate, w_mix)
    cosines, sines = tables(LEN, width // decay_rate.shape[0])
    anywhere = pl.BlockSpec(memory_space=pl.ANY)
    inputs = {"w_" + name: (w, anywhere) for name, w in zip(WEIGHTS, weights)}
    inputs["tok"] = (tokens, vmem())
    inputs["rate"] = (decay_rate[None], pl.BlockSpec(memory_space=pltpu.SMEM))
    inputs["cosines"], inputs["sines"] = (cosines, vmem()), (sines, vmem())
    for name, value in (
        ("gain_one", gain_one), ("gain_mix", gain_mix), ("gain_two", gain_two),
        ("scale_gate", scale_gate), ("scale_up", scale_up), ("scale_down", scale_down),
        ("scale_query", scale_query), ("scale_key", scale_key), ("scale_value", scale_value),
        ("scale_outgate", scale_outgate), ("scale_mix", scale_mix), ("ret_gain", ret_gain),
    ):
        inputs[name] = (value[None], vmem())
    scratch = {}
    for name, w, dim in zip(WEIGHTS, weights, DIMS):
        grown = tuple(size * (nfs if axis == dim else 1) for axis, size in enumerate(w.shape))
        scratch[name] = pltpu.VMEM(grown, BF16)
        scratch["stage_" + name] = pltpu.VMEM(w.shape, F32)
    for i in range(3):
        scratch["full_%d" % i] = pltpu.VMEM((rows, model), BF16)
    scratch["part"] = pltpu.VMEM((rows, model), BF16)
    scratch["hidden"] = pltpu.VMEM((rows, w_gate.shape[1]), BF16)
    far = max(nx - 1, 1)
    scratch["pair"] = pltpu.VMEM((far, rows, width), BF16)
    scratch["one"] = pltpu.VMEM((3, nx, rows, width), BF16)
    scratch["two"] = pltpu.VMEM((3, far, rows, width), BF16)
    for name in ("a_query", "a_key", "a_value", "a_outgate", "mixed", "first", "second"):
        scratch[name] = pltpu.VMEM((rows, width), BF16)
    scratch["gain_own"] = pltpu.VMEM((8, width), F32)
    scratch["gains"] = pltpu.VMEM((8, model), F32)
    total = sum(PARTS)
    scratch["load_sem"] = dma(len(WEIGHTS))
    scratch["w_send"], scratch["w_recv"] = dma(ny + 1, nfs, total), dma(nfs, total)
    scratch["n_send"], scratch["n_fwd"], scratch["n_recv"] = dma(nx, 1), dma(nx, 1), dma(ntp, 1)
    scratch["g_send"], scratch["g_fwd"] = dma(3, nx, count), dma(3, nx, count)
    scratch["g_recv"] = dma(3, ntp, count)
    scratch["r_s1"], scratch["r_v1"] = dma(3, nx, count), dma(3, nx, count)
    scratch["r_s2"], scratch["r_v2"] = dma(3, far, count), dma(3, far, count)
    names = list(inputs) + ["out"] + list(scratch)
    return pl.pallas_call(
        functools.partial(layer_kernel, nfs, ntp, ny, names),
        out_shape=jax.ShapeDtypeStruct((rows, width), BF16),
        in_specs=[spec for _, spec in inputs.values()],
        out_specs=vmem(),
        scratch_shapes=list(scratch.values()),
        compiler_params=pltpu.CompilerParams(
            collective_id=0, has_side_effects=True, vmem_limit_bytes=67043328
        ),
        cost_estimate=pl.CostEstimate(flops=4 * 10**10, bytes_accessed=2**24, transcendentals=0),
        name="layer",
    )(*[value for value, _ in inputs.values()])


def solution(mesh):
    return jax.shard_map(
        functools.partial(per_device, mesh.shape["fs"], mesh.shape["tp"]),
        mesh=mesh,
        in_specs=(
            P("fs", "tp"), P("tp"), P("fs", "tp"), P("fs", "tp"), P("tp", "fs"),
            P("tp"), P("tp"), P("tp"), P("tp"),
            P("fs", "tp"), P("fs", "tp"), P("fs", "tp"), P("fs", "tp"),
            P("tp"), P("tp"), P("tp"), P("tp"), P("tp"), P("tp"),
            P("tp", "fs"), P("tp"), P("tp"),
        ),
        out_specs=P("fs", "tp"),
        check_vma=False,
    )
```

```python
import functools
from types import SimpleNamespace

import jax
import jax.numpy as jnp
import numpy as np
from jax import lax
from jax.experimental import pallas as pl
from jax.experimental.pallas import tpu as pltpu
from jax.sharding import PartitionSpec as P

LEN = 256
EPS = 1e-06
HEAD_EPS = 0.1
MESH = pl.DeviceIdType.MESH
BF16 = jnp.bfloat16
F32 = jnp.float32
WEIGHTS = ("gate", "up", "down", "mix", "query", "key", "value", "outgate")
DIMS = (0, 0, 1, 1, 0, 0, 0, 0)
STAGES = (0, 1, 2, 2, 0, 1, 0, 1)


def cols_at(index, width):
    return pl.ds(pl.multiple_of(index * width, width), width)


def remote(src, dst, send_sem, recv_sem, axis, target):
    return pltpu.make_async_remote_copy(
        src_ref=src,
        dst_ref=dst,
        send_sem=send_sem,
        recv_sem=recv_sem,
        device_id={axis: target},
        device_id_type=MESH,
    )


def dot(left, right):
    return jnp.dot(left, right, preferred_element_type=F32)


class TpGroup:
    def __init__(self, ntp):
        self.ntp, self.nx = ntp, ntp // 2
        self.t = lax.axis_index("tp")
        self.core, self.chip = lax.rem(self.t, 2), lax.div(self.t, 2)
        self.partner = self.chip * 2 + (1 - self.core)

    def along_x(self, offset, core):
        return lax.rem(self.chip + offset, self.nx) * 2 + core

    def greet(self, barrier):
        for offset in range(1, self.ntp):
            target = lax.rem(self.t + offset, self.ntp)
            pl.semaphore_signal(barrier, inc=1, device_id={"tp": target}, device_id_type=MESH)
        return self.ntp - 1


class TpGather:
    def __init__(self, group, out, sems, rows):
        self.group = group
        self.out, self.rows = out, rows
        self.sends, self.forwards, self.recvs = sems
        self.width = out.shape[1] // group.ntp

    def at(self, piece):
        return pl.ds(piece * self.rows, self.rows)

    def place(self, index, piece):
        return self.out.at[self.at(piece), cols_at(index, self.width)]

    def own_sends(self, piece):
        group = self.group
        copies = []
        for offset in range(group.nx - 1, -1, -1):
            target = group.along_x(offset, group.core) if offset else group.partner
            copies.append(
                remote(
                    self.place(group.t, piece), self.place(group.t, piece),
                    self.sends.at[offset, piece], self.recvs.at[group.t, piece], "tp", target,
                )
            )
        return copies

    def forward(self, offset, piece):
        group = self.group
        index = group.along_x(group.nx - offset, group.core)
        block = self.place(index, piece)
        return remote(
            block, block, self.forwards.at[offset, piece], self.recvs.at[index, piece],
            "tp", group.partner,
        )

    def arrived(self, index, piece):
        block = self.place(index, piece)
        remote(
            block, block, self.sends.at[0, piece], self.recvs.at[index, piece],
            "tp", self.group.partner,
        ).wait_recv()

    def start(self, piece):
        for copy in self.own_sends(piece):
            copy.start()

    def relay(self, piece):
        group = self.group
        for offset in range(1, group.nx):
            self.arrived(group.along_x(group.nx - offset, group.core), piece)
            self.forward(offset, piece).start()

    def complete(self, piece):
        group = self.group
        for offset in range(group.nx):
            self.arrived(group.along_x(offset, 1 - group.core), piece)

    def finish(self, piece):
        for copy in self.own_sends(piece):
            copy.wait_send()
        for offset in range(1, self.group.nx):
            self.forward(offset, piece).wait_send()


class TpReduce:
    def __init__(self, group, part, pair, one, two, sems, rows, width):
        self.group, self.part, self.pair, self.one, self.two = group, part, pair, one, two
        self.s1, self.v1, self.s2, self.v2 = sems
        self.rows, self.width = rows, width

    def at(self, piece):
        return pl.ds(piece * self.rows, self.rows)

    def block(self, offset, core):
        return cols_at(self.group.along_x(offset, core), self.width)

    def to_partner(self, offset, piece):
        return remote(
            self.part.at[self.at(piece), self.block(offset, 1 - self.group.core)],
            self.one.at[offset, self.at(piece)],
            self.s1.at[offset, piece], self.v1.at[offset, piece], "tp", self.group.partner,
        )

    def across(self, offset, piece):
        return remote(
            self.pair.at[offset - 1, self.at(piece)],
            self.two.at[offset - 1, self.at(piece)],
            self.s2.at[offset - 1, piece], self.v2.at[offset - 1, piece],
            "tp", self.group.along_x(offset, self.group.core),
        )

    def start(self, piece):
        for offset in range(self.group.nx - 1, -1, -1):
            self.to_partner(offset, piece).start()

    def cross(self, piece):
        at = self.at(piece)
        for offset in range(self.group.nx - 1, 0, -1):
            self.to_partner(offset, piece).wait_recv()
            mine = self.part[at, self.block(offset, self.group.core)].astype(F32)
            self.pair[offset - 1, at] = (mine + self.one[offset, at].astype(F32)).astype(BF16)
            self.across(offset, piece).start()

    def total(self, piece):
        at = self.at(piece)
        self.to_partner(0, piece).wait_recv()
        value = self.part[at, self.block(0, self.group.core)].astype(F32)
        value = value + self.one[0, at].astype(F32)
        for offset in range(1, self.group.nx):
            self.across(offset, piece).wait_recv()
            value = value + self.two[offset - 1, at].astype(F32)
        return value

    def finish(self, piece):
        for offset in range(self.group.nx):
            self.to_partner(offset, piece).wait_send()
        for offset in range(1, self.group.nx):
            self.across(offset, piece).wait_send()


class FsStream:
    def __init__(self, nfs, ny, pieces, sends, recvs):
        self.ny, self.nz = ny, nfs // ny
        self.f = lax.axis_index("fs")
        self.z, self.y = lax.div(self.f, ny), lax.rem(self.f, ny)
        self.pieces = pieces
        self.sends, self.recvs = sends, recvs
        self.events, self.done = self.schedule(), 0

    def whole_z(self, p):
        return self.pieces[p].along_z

    def place(self, p, index):
        piece = self.pieces[p]
        if piece.dim == 0:
            start = pl.multiple_of(index * piece.rows + piece.start, 16)
            return piece.buf.at[pl.ds(start, piece.size)]
        return piece.buf.at[pl.ds(piece.start, piece.size), cols_at(index, piece.cols)]

    def move(self, p, kind, index, target):
        block = self.place(p, index)
        return remote(
            block, block, self.sends.at[kind, index, p], self.recvs.at[index, p], "fs", target
        )

    def arrived(self, p, index):
        self.move(p, 0, index, self.f).wait_recv()

    def move_z(self, p, step, index, act):
        inside = (self.z < self.nz - 1) if step > 0 else (self.z > 0)

        @pl.when(inside)
        def _():
            act(self.move(p, 0 if step > 0 else 1, index, self.f + step * self.ny))

    def move_y(self, p, index, act):
        for offset in range(1, self.ny):
            target = self.z * self.ny + lax.rem(self.y + offset, self.ny)
            act(self.move(p, 1 + offset, index, target))

    def others(self, zs):
        return [zs * self.ny + lax.rem(self.y + offset, self.ny) for offset in range(1, self.ny)]

    def own(self, p, act, wait):
        self.move_y(p, self.f, act)
        for step in (1, -1):
            self.move_z(p, step, self.f, act)

    def side(self, p, act, wait):
        for index in self.others(self.z):
            if wait:
                self.arrived(p, index)
            for step in (1, -1):
                self.move_z(p, step, index, act)

    def relay(self, distance, p, act, wait):
        for step in (1, -1):
            zs = self.z - step * distance

            @pl.when(jnp.logical_and(zs >= 0, zs < self.nz))
            def _():
                same = zs * self.ny + self.y
                for index in [same] + (self.others(zs) if self.whole_z(p) else []):
                    if wait:
                        self.arrived(p, index)
                    self.move_z(p, step, index, act)
                    if not self.whole_z(p):
                        self.move_y(p, index, act)

    def schedule(self):
        events = []
        for p in range(len(self.pieces)):
            late = self.whole_z(p)
            events.append((p - 1.3 + 0.5 * late, p, functools.partial(self.own, p)))
            if late:
                events.append((p + 1.2, p, functools.partial(self.side, p)))
            for distance in range(1, self.nz):
                when = p + 0.75 * distance + (1.55 if late else -0.4)
                events.append((when, p, functools.partial(self.relay, distance, p)))
        events.sort(key=lambda event: event[:2])
        return [event[1:] for event in events]

    def some(self, count):
        for _, event in self.events[self.done : self.done + count]:
            event(lambda copy: copy.start(), True)
        self.done = min(self.done + count, len(self.events))

    def need(self, p):
        last = max(i for i, (piece, _) in enumerate(self.events) if piece == p)
        self.some(max(0, last + 1 - self.done))
        if not self.whole_z(p):
            for zs in range(self.nz):
                for index in self.others(zs):
                    self.arrived(p, index)

    def finish(self):
        for _, event in self.events:
            event(lambda copy: copy.wait_send(), False)

    def greet(self, barrier):
        ny, z, f = self.ny, self.z, self.f
        for index in self.others(z):
            pl.semaphore_signal(barrier, inc=1, device_id={"fs": index}, device_id_type=MESH)

        @pl.when(z > 0)
        def _():
            pl.semaphore_signal(barrier, inc=1, device_id={"fs": f - ny}, device_id_type=MESH)

        @pl.when(z < self.nz - 1)
        def _():
            pl.semaphore_signal(barrier, inc=1, device_id={"fs": f + ny}, device_id_type=MESH)

        ends = (z > 0).astype(jnp.int32) + (z < self.nz - 1).astype(jnp.int32)
        return ends + (ny - 1)


def layer_kernel(nfs, ntp, ny, names, *refs):
    r = SimpleNamespace(**dict(zip(names, refs)))
    rows, width = r.out.shape
    model = width * ntp
    half = model // 2
    count = rows // LEN
    chunks = range(count)
    group = TpGroup(ntp)
    shards = [getattr(r, "w_" + name) for name in WEIGHTS]
    wholes = [getattr(r, name) for name in WEIGHTS]
    pieces, held = [], {name: [] for name in WEIGHTS}
    for i, name in enumerate(WEIGHTS):
        height, cols = shards[i].shape
        along_z = max(16, height * 3 // 16 // 16 * 16)
        for late, start, size in ((True, 0, along_z), (False, along_z, height - along_z)):
            held[name].append(len(pieces))
            pieces.append(
                SimpleNamespace(
                    buf=wholes[i], dim=DIMS[i], rows=height, cols=cols,
                    start=start, size=size, along_z=late,
                )
            )
    stream = FsStream(nfs, ny, pieces, r.w_send, r.w_recv)

    def need(name):
        for p in held[name]:
            stream.need(p)

    def at(c):
        return pl.ds(c * LEN, LEN)

    own = cols_at(group.t, width)
    mine = cols_at(group.core, half)
    stages = [r.stage_0, r.stage_1, r.stage_2]

    def load(i):
        height, cols = shards[i].shape
        stage = stages[STAGES[i]].at[pl.ds(0, height), pl.ds(0, cols)]
        return pltpu.make_async_copy(shards[i], stage, r.load_sem.at[i])

    def cast(i):
        load(i).wait()
        height, cols = shards[i].shape
        value = stages[STAGES[i]][0:height, 0:cols].astype(BF16)
        if DIMS[i] == 0:
            wholes[i][pl.ds(pl.multiple_of(stream.f * height, height), height), :] = value
        else:
            wholes[i][:, cols_at(stream.f, cols)] = value

    barrier = pltpu.get_barrier_semaphore()
    greeted = group.greet(barrier) + stream.greet(barrier)
    tok_load = pltpu.make_async_copy(r.tok, r.full_0.at[:, own], r.tok_sem)
    table_loads = [
        pltpu.make_async_copy(src, dst, r.table_sem.at[i])
        for i, (src, dst) in enumerate(((r.cosines, r.cos), (r.sines, r.sin)))
    ]
    load(0).start()
    tok_load.start()
    load(1).start()
    load(2).start()
    for table in table_loads:
        table.start()
    r.gain_own[...] = jnp.zeros(r.gain_own.shape, F32)
    for row, ref in enumerate((r.gain_one, r.gain_mix, r.gain_two, r.scale_mix)):
        r.gain_own[row : row + 1, :] = ref[...]
    r.gains[:, own] = r.gain_own[...]
    for src, dst in ((r.scale_gate, r.s_gate), (r.scale_up, r.s_up)):
        for row in range(src.shape[0]):
            dst[:, row * 128 : (row + 1) * 128] = src[row : row + 1, :]
    cast(0)
    pl.semaphore_wait(barrier, greeted)

    gain_gather = TpGather(group, r.gains, (r.n_send, r.n_fwd, r.n_recv), 8)
    gathers = [
        TpGather(group, full, (r.g_send.at[i], r.g_fwd.at[i], r.g_recv.at[i]), LEN)
        for i, full in enumerate((r.full_0, r.full_1, r.mixed))
    ]
    reduces = [
        TpReduce(
            group, r.part, r.pair, r.one.at[i], r.two.at[i],
            (r.r_s1.at[i], r.r_v1.at[i], r.r_s2.at[i], r.r_v2.at[i]), LEN, width,
        )
        for i in range(2)
    ]
    stream.some(2)
    gain_gather.start(0)
    tok_load.wait()
    for c in chunks:
        gathers[0].start(c)
    cast(1)
    load(4).start()
    load(5).start()
    cast(2)
    load(3).start()
    stream.some(2)
    cast(3)
    cast(4)
    load(6).start()
    cast(5)
    load(7).start()
    cast(6)
    cast(7)

    def norm(full, row, c):
        gain = r.gains[row : row + 1, :]
        step = 32

        def body(i, carry):
            some = pl.ds(pl.multiple_of(c * LEN + i * step, step), step)
            v = full[some, :].astype(F32)
            mean = jnp.mean(v * v, axis=1, keepdims=True)
            r.normed[some, :] = (v * lax.rsqrt(mean + EPS) * gain).astype(BF16)
            return carry

        lax.fori_loop(0, LEN // step, body, 0)

    def gate_up(c):
        units = r.gate.shape[1]
        tile = 256 if units % 256 == 0 else 128

        def body(n, carry):
            cols = cols_at(n, tile)
            x = r.normed[at(c), :]
            g = dot(x, r.gate[:, cols]) * r.s_gate[:, cols]
            u = dot(x, r.up[:, cols]) * r.s_up[:, cols]
            r.hidden[at(c), cols] = (g / (1.0 + jnp.exp(-g)) * u).astype(BF16)
            return carry

        lax.fori_loop(0, units // tile, body, 0)

    def partial(c):
        def body(n, carry):
            cols = cols_at(n, width)
            r.part[at(c), cols] = dot(r.hidden[at(c), :], r.down[:, cols]).astype(BF16)
            return carry

        lax.fori_loop(0, ntp, body, 0)

    def project(name):
        weight, scale, out = getattr(r, name), getattr(r, "scale_" + name), getattr(r, "a_" + name)

        def body(c, carry):
            some = pl.ds(pl.multiple_of(c * LEN, LEN), LEN)
            out[some, :] = (dot(r.normed[some, :], weight[...]) * scale[...]).astype(BF16)
            return carry

        lax.fori_loop(0, count, body, 0)

    heads = r.rate.shape[1]
    size = width // heads

    def retain(c):
        even = lax.rem(lax.broadcasted_iota(jnp.int32, (LEN, size), 1), 2) == 0
        distance = lax.broadcasted_iota(jnp.int32, (LEN, LEN), 0) - lax.broadcasted_iota(
            jnp.int32, (LEN, LEN), 1
        )

        def body(h, carry):
            cols = cols_at(h, size)

            def turned(ref):
                v = ref[at(c), cols].astype(F32)
                swapped = jnp.where(even, -pltpu.roll(v, size - 1, 1), pltpu.roll(v, 1, 1))
                return v * r.cos[...] + swapped * r.sin[...]

            q = turned(r.a_query).astype(BF16)
            k = (turned(r.a_key) * size ** -0.5).astype(BF16)
            scores = lax.dot_general(q, k, (((1,), (1,)), ((), ())), preferred_element_type=F32)
            decay = jnp.exp(-r.rate[0, h] * jnp.maximum(distance, 0).astype(F32))
            scores = jnp.where(distance >= 0, scores * decay, 0.0).astype(BF16)
            kept = dot(scores, r.a_value[at(c), cols])
            kept = kept * lax.rsqrt(jnp.mean(kept * kept, axis=1, keepdims=True) + HEAD_EPS)
            r.kept[at(c), cols] = kept * r.ret_gain[:, cols]
            return carry

        lax.fori_loop(0, heads, body, 0)

    def gated(c):
        g = dot(r.normed[at(c), :], r.outgate[...]) * r.scale_outgate[...]
        g = g.astype(BF16).astype(F32)
        r.mixed[at(c), own] = (r.kept[at(c), :] * (g / (1.0 + jnp.exp(-g)))).astype(BF16)

    def spread_mix(offset):
        target = lax.rem(group.t + offset, ntp)
        there = cols_at(lax.rem(target, 2), half)
        place = pl.ds(pl.multiple_of(group.t * width, width), width)
        return remote(
            r.mix.at[:, there], r.mix_all.at[place], r.x_send.at[offset], r.x_recv.at[group.t],
            "tp", target,
        )

    def mix_arrived(offset):
        source = lax.rem(group.t + offset, ntp)
        place = pl.ds(pl.multiple_of(source * width, width), width)
        remote(
            r.mix.at[:, mine], r.mix_all.at[place], r.x_send.at[offset], r.x_recv.at[source],
            "tp", source,
        ).wait_recv()

    def swap(c):
        block = r.full_2.at[at(c), mine]
        return remote(block, block, r.h_send.at[c], r.h_recv.at[c], "tp", group.partner)

    def swapped(c):
        block = r.full_2.at[at(c), cols_at(1 - group.core, half)]
        remote(block, block, r.h_send.at[c], r.h_recv.at[c], "tp", group.partner).wait_recv()

    def second(c):
        tile = 512

        def body(n, carry):
            cols = cols_at(n, tile)
            there = pl.ds(pl.multiple_of(group.core * half + n * tile, tile), tile)
            total = dot(r.mixed[at(c), :], r.mix_all[:, cols]) * r.gains[3:4, there]
            r.full_2[at(c), there] = (r.full_1[at(c), there].astype(F32) + total).astype(BF16)
            return carry

        lax.fori_loop(0, half // tile, body, 0)

    def settle(i, c, res, out, place):
        value = res[at(c), own].astype(F32)
        value = value + 0.5 * reduces[i].total(c) * r.scale_down[...]
        out[at(c), place] = value.astype(BF16)

    gain_gather.relay(0)
    for c in chunks:
        stream.some(3)
        gathers[0].relay(c)
    gain_gather.complete(0)
    for c in chunks:
        stream.some(1)
        gathers[0].complete(c)
        norm(r.full_0, 0, c)
    need("gate")
    need("up")
    for c in chunks:
        gate_up(c)
        stream.some(1)
    need("down")
    for c in chunks:
        partial(c)
        reduces[0].start(c)
        stream.some(1)
    for c in chunks:
        reduces[0].cross(c)
        stream.some(1)
    for c in chunks:
        settle(0, c, r.full_0, r.full_1, own)
        gathers[1].start(c)
        stream.some(1)
    need("mix")
    for offset in range(1, ntp):
        spread_mix(offset).start()
    r.mix_all[pl.ds(pl.multiple_of(group.t * width, width), width), :] = r.mix[:, mine]
    for c in chunks:
        gathers[1].relay(c)
        stream.some(1)
    for c in chunks:
        gathers[1].complete(c)
        norm(r.full_1, 1, c)
        reduces[0].finish(c)
        stream.some(1)
    for table in table_loads:
        table.wait()
    for name in ("query", "key", "value"):
        need(name)
        project(name)
        stream.some(1)
    for c in chunks:
        retain(c)
        stream.some(1)
    for offset in range(1, ntp):
        mix_arrived(offset)
    need("outgate")
    for c in chunks:
        gated(c)
        gathers[2].start(c)
    gathers[2].relay(0)
    for c in chunks:
        gathers[2].complete(c)
        second(c)
        swap(c).start()
        if c > 0:
            reduces[1].cross(c - 1)
        if c + 1 < count:
            gathers[2].relay(c + 1)
        swapped(c)
        norm(r.full_2, 2, c)
        gate_up(c)
        partial(c)
        reduces[1].start(c)
    reduces[1].cross(count - 1)
    for c in chunks:
        settle(1, c, r.full_2, r.out, pl.ds(0, width))
    for c in chunks:
        reduces[1].finish(c)
        swap(c).wait_send()
        for gather in gathers:
            gather.finish(c)
    for offset in range(1, ntp):
        spread_mix(offset).wait_send()
    gain_gather.finish(0)
    stream.finish()


def vmem():
    return pl.BlockSpec(memory_space=pltpu.VMEM)


def dma(*shape):
    return pltpu.SemaphoreType.DMA(shape)


def along_y_of(nfs, ntp):
    return ntp // 2 if nfs % (ntp // 2) == 0 else 1


def tables(length, width):
    freq = np.float32(1.0) / np.float32(10000.0) ** np.linspace(0.0, 1.0, width // 2, dtype=np.float32)
    angles = np.arange(length, dtype=np.float32)[:, None] * np.repeat(freq, 2)[None, :]
    return jnp.asarray(np.cos(angles)), jnp.asarray(np.sin(angles))


def per_device(
    nfs, ntp,
    tokens, gain_one, w_gate, w_up, w_down, scale_gate, scale_up, scale_down,
    gain_mix, w_query, w_key, w_value, w_outgate,
    scale_query, scale_key, scale_value, scale_outgate,
    ret_gain, decay_rate, w_mix, scale_mix, gain_two,
):
    ny, nx = along_y_of(nfs, ntp), ntp // 2
    rows, width = tokens.shape
    count = rows // LEN
    model = width * ntp
    weights = (w_gate, w_up, w_down, w_mix, w_query, w_key, w_value, w_outgate)
    cosines, sines = tables(LEN, width // decay_rate.shape[0])
    anywhere = pl.BlockSpec(memory_space=pl.ANY)
    inputs = {"w_" + name: (w, anywhere) for name, w in zip(WEIGHTS, weights)}
    inputs["tok"] = (tokens, anywhere)
    inputs["rate"] = (decay_rate[None], pl.BlockSpec(memory_space=pltpu.SMEM))
    inputs["cosines"], inputs["sines"] = (cosines, anywhere), (sines, anywhere)
    inputs["scale_gate"] = (scale_gate.reshape(-1, 128), vmem())
    inputs["scale_up"] = (scale_up.reshape(-1, 128), vmem())
    for name, value in (
        ("gain_one", gain_one), ("gain_mix", gain_mix), ("gain_two", gain_two),
        ("scale_down", scale_down), ("scale_query", scale_query), ("scale_key", scale_key),
        ("scale_value", scale_value), ("scale_outgate", scale_outgate),
        ("scale_mix", scale_mix), ("ret_gain", ret_gain),
    ):
        inputs[name] = (value[None], vmem())
    scratch = {}
    for name, w, dim in zip(WEIGHTS, weights, DIMS):
        grown = tuple(size * (nfs if axis == dim else 1) for axis, size in enumerate(w.shape))
        scratch[name] = pltpu.VMEM(grown, BF16)
    for i in range(3):
        shapes = [w.shape for w, stage in zip(weights, STAGES) if stage == i]
        scratch["stage_%d" % i] = pltpu.VMEM(tuple(max(sizes) for sizes in zip(*shapes)), F32)
    for name in ("full_0", "full_1", "full_2", "normed", "mixed", "part"):
        scratch[name] = pltpu.VMEM((rows, model), BF16)
    scratch["mix_all"] = pltpu.VMEM((model, model // 2), BF16)
    scratch["hidden"] = pltpu.VMEM((rows, w_gate.shape[1]), BF16)
    far = max(nx - 1, 1)
    scratch["pair"] = pltpu.VMEM((far, rows, width), BF16)
    scratch["one"] = pltpu.VMEM((2, nx, rows, width), BF16)
    scratch["two"] = pltpu.VMEM((2, far, rows, width), BF16)
    for name in ("a_query", "a_key", "a_value"):
        scratch[name] = pltpu.VMEM((rows, width), BF16)
    scratch["kept"] = pltpu.VMEM((rows, width), F32)
    scratch["cos"], scratch["sin"] = pltpu.VMEM(cosines.shape, F32), pltpu.VMEM(sines.shape, F32)
    scratch["s_gate"] = pltpu.VMEM((1, w_gate.shape[1]), F32)
    scratch["s_up"] = pltpu.VMEM((1, w_up.shape[1]), F32)
    scratch["gain_own"] = pltpu.VMEM((8, width), F32)
    scratch["gains"] = pltpu.VMEM((8, model), F32)
    total = 2 * len(WEIGHTS)
    scratch["load_sem"], scratch["tok_sem"] = dma(len(WEIGHTS)), dma()
    scratch["table_sem"] = dma(2)
    scratch["w_send"], scratch["w_recv"] = dma(ny + 1, nfs, total), dma(nfs, total)
    scratch["n_send"], scratch["n_fwd"], scratch["n_recv"] = dma(nx, 1), dma(nx, 1), dma(ntp, 1)
    scratch["g_send"], scratch["g_fwd"] = dma(3, nx, count), dma(3, nx, count)
    scratch["g_recv"] = dma(3, ntp, count)
    scratch["r_s1"], scratch["r_v1"] = dma(2, nx, count), dma(2, nx, count)
    scratch["r_s2"], scratch["r_v2"] = dma(2, far, count), dma(2, far, count)
    scratch["x_send"], scratch["x_recv"] = dma(ntp), dma(ntp)
    scratch["h_send"], scratch["h_recv"] = dma(count), dma(count)
    names = list(inputs) + ["out"] + list(scratch)
    return pl.pallas_call(
        functools.partial(layer_kernel, nfs, ntp, ny, names),
        out_shape=jax.ShapeDtypeStruct((rows, width), BF16),
        in_specs=[spec for _, spec in inputs.values()],
        out_specs=vmem(),
        scratch_shapes=list(scratch.values()),
        compiler_params=pltpu.CompilerParams(
            collective_id=0, has_side_effects=True, vmem_limit_bytes=67043328
        ),
        cost_estimate=pl.CostEstimate(flops=4 * 10**10, bytes_accessed=2**24, transcendentals=0),
        name="layer",
    )(*[value for value, _ in inputs.values()])


def solution(mesh):
    return jax.shard_map(
        functools.partial(per_device, mesh.shape["fs"], mesh.shape["tp"]),
        mesh=mesh,
        in_specs=(
            P("fs", "tp"), P("tp"), P("fs", "tp"), P("fs", "tp"), P("tp", "fs"),
            P("tp"), P("tp"), P("tp"), P("tp"),
            P("fs", "tp"), P("fs", "tp"), P("fs", "tp"), P("fs", "tp"),
            P("tp"), P("tp"), P("tp"), P("tp"), P("tp"), P("tp"),
            P("tp", "fs"), P("tp"), P("tp"),
        ),
        out_specs=P("fs", "tp"),
        check_vma=False,
    )
```

```python
import functools
from types import SimpleNamespace

import jax
import jax.numpy as jnp
import numpy as np
from jax import lax
from jax.experimental import pallas as pl
from jax.experimental.pallas import tpu as pltpu
from jax.sharding import PartitionSpec as P

LEN = 256
EPS = 1e-06
HEAD_EPS = 0.1
MESH = pl.DeviceIdType.MESH
BF16 = jnp.bfloat16
F32 = jnp.float32
WEIGHTS = ("gate", "up", "down", "mix", "query", "key", "value", "outgate")
DIMS = (0, 0, 1, 1, 0, 0, 0, 0)
STAGES = (0, 1, 2, 2, 0, 1, 0, 1)


def cols_at(index, width):
    return pl.ds(pl.multiple_of(index * width, width), width)


def remote(src, dst, send_sem, recv_sem, axis, target):
    return pltpu.make_async_remote_copy(
        src_ref=src,
        dst_ref=dst,
        send_sem=send_sem,
        recv_sem=recv_sem,
        device_id={axis: target},
        device_id_type=MESH,
    )


def dot(left, right):
    return jnp.dot(left, right, preferred_element_type=F32)


class TpGroup:
    def __init__(self, ntp):
        self.ntp, self.nx = ntp, ntp // 2
        self.t = lax.axis_index("tp")
        self.core, self.chip = lax.rem(self.t, 2), lax.div(self.t, 2)
        self.partner = self.chip * 2 + (1 - self.core)

    def along_x(self, offset, core):
        return lax.rem(self.chip + offset, self.nx) * 2 + core

    def greet(self, barrier):
        for offset in range(1, self.ntp):
            target = lax.rem(self.t + offset, self.ntp)
            pl.semaphore_signal(barrier, inc=1, device_id={"tp": target}, device_id_type=MESH)
        return self.ntp - 1


class TpGather:
    def __init__(self, group, out, sems, rows):
        self.group = group
        self.out, self.rows = out, rows
        self.sends, self.forwards, self.recvs = sems
        self.width = out.shape[1] // group.ntp

    def at(self, piece):
        return pl.ds(piece * self.rows, self.rows)

    def place(self, index, piece):
        return self.out.at[self.at(piece), cols_at(index, self.width)]

    def own_sends(self, piece):
        group = self.group
        copies = []
        for offset in range(group.nx - 1, -1, -1):
            target = group.along_x(offset, group.core) if offset else group.partner
            copies.append(
                remote(
                    self.place(group.t, piece), self.place(group.t, piece),
                    self.sends.at[offset, piece], self.recvs.at[group.t, piece], "tp", target,
                )
            )
        return copies

    def forward(self, offset, piece):
        group = self.group
        index = group.along_x(group.nx - offset, group.core)
        block = self.place(index, piece)
        return remote(
            block, block, self.forwards.at[offset, piece], self.recvs.at[index, piece],
            "tp", group.partner,
        )

    def arrived(self, index, piece):
        block = self.place(index, piece)
        remote(
            block, block, self.sends.at[0, piece], self.recvs.at[index, piece],
            "tp", self.group.partner,
        ).wait_recv()

    def start(self, piece):
        for copy in self.own_sends(piece):
            copy.start()

    def relay(self, piece):
        group = self.group
        for offset in range(1, group.nx):
            self.arrived(group.along_x(group.nx - offset, group.core), piece)
            self.forward(offset, piece).start()

    def complete(self, piece):
        group = self.group
        for offset in range(group.nx):
            self.arrived(group.along_x(offset, 1 - group.core), piece)

    def finish(self, piece):
        for copy in self.own_sends(piece):
            copy.wait_send()
        for offset in range(1, self.group.nx):
            self.forward(offset, piece).wait_send()


class TpReduce:
    def __init__(self, group, part, pair, one, two, sems, rows, width):
        self.group, self.part, self.pair, self.one, self.two = group, part, pair, one, two
        self.s1, self.v1, self.s2, self.v2 = sems
        self.rows, self.width = rows, width

    def at(self, piece):
        return pl.ds(piece * self.rows, self.rows)

    def block(self, offset, core):
        return cols_at(self.group.along_x(offset, core), self.width)

    def to_partner(self, offset, piece):
        return remote(
            self.part.at[self.at(piece), self.block(offset, 1 - self.group.core)],
            self.one.at[offset, self.at(piece)],
            self.s1.at[offset, piece], self.v1.at[offset, piece], "tp", self.group.partner,
        )

    def across(self, offset, piece):
        return remote(
            self.pair.at[offset - 1, self.at(piece)],
            self.two.at[offset - 1, self.at(piece)],
            self.s2.at[offset - 1, piece], self.v2.at[offset - 1, piece],
            "tp", self.group.along_x(offset, self.group.core),
        )

    def start(self, piece):
        for offset in range(self.group.nx - 1, -1, -1):
            self.to_partner(offset, piece).start()

    def cross(self, piece):
        at = self.at(piece)
        for offset in range(self.group.nx - 1, 0, -1):
            self.to_partner(offset, piece).wait_recv()
            mine = self.part[at, self.block(offset, self.group.core)].astype(F32)
            self.pair[offset - 1, at] = (mine + self.one[offset, at].astype(F32)).astype(BF16)
            self.across(offset, piece).start()

    def total(self, piece):
        at = self.at(piece)
        self.to_partner(0, piece).wait_recv()
        value = self.part[at, self.block(0, self.group.core)].astype(F32)
        value = value + self.one[0, at].astype(F32)
        for offset in range(1, self.group.nx):
            self.across(offset, piece).wait_recv()
            value = value + self.two[offset - 1, at].astype(F32)
        return value

    def finish(self, piece):
        for offset in range(self.group.nx):
            self.to_partner(offset, piece).wait_send()
        for offset in range(1, self.group.nx):
            self.across(offset, piece).wait_send()


class FsStream:
    def __init__(self, nfs, ny, pieces, sends, recvs):
        self.ny, self.nz = ny, nfs // ny
        self.f = lax.axis_index("fs")
        self.z, self.y = lax.div(self.f, ny), lax.rem(self.f, ny)
        self.pieces = pieces
        self.sends, self.recvs = sends, recvs
        self.events, self.done = self.schedule(), 0

    def whole_z(self, p):
        return self.pieces[p].along_z

    def place(self, p, index):
        piece = self.pieces[p]
        if piece.dim == 0:
            start = pl.multiple_of(index * piece.rows + piece.start, 16)
            return piece.buf.at[pl.ds(start, piece.size)]
        return piece.buf.at[pl.ds(piece.start, piece.size), cols_at(index, piece.cols)]

    def move(self, p, kind, index, target):
        block = self.place(p, index)
        return remote(
            block, block, self.sends.at[kind, index, p], self.recvs.at[index, p], "fs", target
        )

    def arrived(self, p, index):
        self.move(p, 0, index, self.f).wait_recv()

    def move_z(self, p, step, index, act):
        inside = (self.z < self.nz - 1) if step > 0 else (self.z > 0)

        @pl.when(inside)
        def _():
            act(self.move(p, 0 if step > 0 else 1, index, self.f + step * self.ny))

    def move_y(self, p, index, act):
        for offset in range(1, self.ny):
            target = self.z * self.ny + lax.rem(self.y + offset, self.ny)
            act(self.move(p, 1 + offset, index, target))

    def others(self, zs):
        return [zs * self.ny + lax.rem(self.y + offset, self.ny) for offset in range(1, self.ny)]

    def own(self, p, act, wait):
        self.move_y(p, self.f, act)
        for step in (1, -1):
            self.move_z(p, step, self.f, act)

    def side(self, p, act, wait):
        for index in self.others(self.z):
            if wait:
                self.arrived(p, index)
            for step in (1, -1):
                self.move_z(p, step, index, act)

    def relay(self, distance, p, act, wait):
        for step in (1, -1):
            zs = self.z - step * distance

            @pl.when(jnp.logical_and(zs >= 0, zs < self.nz))
            def _():
                same = zs * self.ny + self.y
                for index in [same] + (self.others(zs) if self.whole_z(p) else []):
                    if wait:
                        self.arrived(p, index)
                    self.move_z(p, step, index, act)
                    if not self.whole_z(p):
                        self.move_y(p, index, act)

    def schedule(self):
        events = []
        for p in range(len(self.pieces)):
            late = self.whole_z(p)
            events.append((p - 1.3 + 0.5 * late, p, functools.partial(self.own, p)))
            if late:
                events.append((p + 1.2, p, functools.partial(self.side, p)))
            for distance in range(1, self.nz):
                when = p + 0.75 * distance + (1.55 if late else -0.4)
                events.append((when, p, functools.partial(self.relay, distance, p)))
        events.sort(key=lambda event: event[:2])
        return [event[1:] for event in events]

    def some(self, count):
        for _, event in self.events[self.done : self.done + count]:
            event(lambda copy: copy.start(), True)
        self.done = min(self.done + count, len(self.events))

    def need(self, p):
        last = max(i for i, (piece, _) in enumerate(self.events) if piece == p)
        self.some(max(0, last + 1 - self.done))
        if not self.whole_z(p):
            for zs in range(self.nz):
                for index in self.others(zs):
                    self.arrived(p, index)

    def finish(self):
        for _, event in self.events:
            event(lambda copy: copy.wait_send(), False)

    def greet(self, barrier):
        ny, z, f = self.ny, self.z, self.f
        for index in self.others(z):
            pl.semaphore_signal(barrier, inc=1, device_id={"fs": index}, device_id_type=MESH)

        @pl.when(z > 0)
        def _():
            pl.semaphore_signal(barrier, inc=1, device_id={"fs": f - ny}, device_id_type=MESH)

        @pl.when(z < self.nz - 1)
        def _():
            pl.semaphore_signal(barrier, inc=1, device_id={"fs": f + ny}, device_id_type=MESH)

        ends = (z > 0).astype(jnp.int32) + (z < self.nz - 1).astype(jnp.int32)
        return ends + (ny - 1)


def layer_kernel(nfs, ntp, ny, names, *refs):
    r = SimpleNamespace(**dict(zip(names, refs)))
    rows, width = r.out.shape
    model = width * ntp
    half = model // 2
    count = rows // LEN
    chunks = range(count)
    group = TpGroup(ntp)
    shards = [getattr(r, "w_" + name) for name in WEIGHTS]
    wholes = [getattr(r, name) for name in WEIGHTS]
    pieces, held = [], {name: [] for name in WEIGHTS}
    for i, name in enumerate(WEIGHTS):
        height, cols = shards[i].shape
        along_z = max(16, height * 3 // 16 // 16 * 16)
        for late, start, size in ((True, 0, along_z), (False, along_z, height - along_z)):
            held[name].append(len(pieces))
            pieces.append(
                SimpleNamespace(
                    buf=wholes[i], dim=DIMS[i], rows=height, cols=cols,
                    start=start, size=size, along_z=late,
                )
            )
    stream = FsStream(nfs, ny, pieces, r.w_send, r.w_recv)

    def need(name):
        for p in held[name]:
            stream.need(p)

    def at(c):
        return pl.ds(c * LEN, LEN)

    own = cols_at(group.t, width)
    mine = cols_at(group.core, half)
    stages = [r.stage_0, r.stage_1, r.stage_2]

    def load(i):
        height, cols = shards[i].shape
        stage = stages[STAGES[i]].at[pl.ds(0, height), pl.ds(0, cols)]
        return pltpu.make_async_copy(shards[i], stage, r.load_sem.at[i])

    def cast(i):
        load(i).wait()
        height, cols = shards[i].shape
        value = stages[STAGES[i]][0:height, 0:cols].astype(BF16)
        if DIMS[i] == 0:
            wholes[i][pl.ds(pl.multiple_of(stream.f * height, height), height), :] = value
        else:
            wholes[i][:, cols_at(stream.f, cols)] = value

    barrier = pltpu.get_barrier_semaphore()
    greeted = group.greet(barrier) + stream.greet(barrier)
    tok_load = pltpu.make_async_copy(r.tok, r.full_0.at[:, own], r.tok_sem)
    table_loads = [
        pltpu.make_async_copy(src, dst, r.table_sem.at[i])
        for i, (src, dst) in enumerate(((r.cosines, r.cos), (r.sines, r.sin)))
    ]
    load(0).start()
    tok_load.start()
    load(1).start()
    load(2).start()
    for table in table_loads:
        table.start()
    r.gain_own[...] = jnp.zeros(r.gain_own.shape, F32)
    for row, ref in enumerate((r.gain_one, r.gain_mix, r.gain_two, r.scale_mix)):
        r.gain_own[row : row + 1, :] = ref[...]
    r.gains[:, own] = r.gain_own[...]
    for src, dst in ((r.scale_gate, r.s_gate), (r.scale_up, r.s_up)):
        for row in range(src.shape[0]):
            dst[:, row * 128 : (row + 1) * 128] = src[row : row + 1, :]
    cast(0)
    pl.semaphore_wait(barrier, greeted)

    gain_gather = TpGather(group, r.gains, (r.n_send, r.n_fwd, r.n_recv), 8)
    gathers = [
        TpGather(group, full, (r.g_send.at[i], r.g_fwd.at[i], r.g_recv.at[i]), LEN)
        for i, full in enumerate((r.full_0, r.full_1, r.mixed))
    ]
    reduces = [
        TpReduce(
            group, r.part, r.pair, r.one.at[i], r.two.at[i],
            (r.r_s1.at[i], r.r_v1.at[i], r.r_s2.at[i], r.r_v2.at[i]), LEN, width,
        )
        for i in range(2)
    ]
    stream.some(2)
    gain_gather.start(0)
    tok_load.wait()
    for c in chunks:
        gathers[0].start(c)
    cast(1)
    load(4).start()
    load(5).start()
    cast(2)
    load(3).start()
    stream.some(2)
    cast(3)
    cast(4)
    load(6).start()
    cast(5)
    load(7).start()
    cast(6)
    cast(7)

    def norm(full, row, c):
        gain = r.gains[row : row + 1, :]
        step = 32

        def body(i, carry):
            some = pl.ds(pl.multiple_of(c * LEN + i * step, step), step)
            v = full[some, :].astype(F32)
            mean = jnp.mean(v * v, axis=1, keepdims=True)
            r.normed[some, :] = (v * lax.rsqrt(mean + EPS) * gain).astype(BF16)
            return carry

        lax.fori_loop(0, LEN // step, body, 0, unroll=4)

    def gate_up(c):
        x = r.normed[at(c), :]
        g = dot(x, r.gate[...]) * r.s_gate[...]
        u = dot(x, r.up[...]) * r.s_up[...]
        r.hidden[at(c), :] = (g / (1.0 + jnp.exp(-g)) * u).astype(BF16)

    def partial(c):
        def body(n, carry):
            cols = cols_at(n, width)
            r.part[at(c), cols] = dot(r.hidden[at(c), :], r.down[:, cols]).astype(BF16)
            return carry

        lax.fori_loop(0, ntp, body, 0)

    def project(name):
        weight, scale, out = getattr(r, name), getattr(r, "scale_" + name), getattr(r, "a_" + name)

        def body(c, carry):
            some = pl.ds(pl.multiple_of(c * LEN, LEN), LEN)
            out[some, :] = (dot(r.normed[some, :], weight[...]) * scale[...]).astype(BF16)
            return carry

        lax.fori_loop(0, count, body, 0)

    heads = r.rate.shape[1]
    size = width // heads

    def retain(c):
        even = lax.rem(lax.broadcasted_iota(jnp.int32, (LEN, size), 1), 2) == 0
        distance = lax.broadcasted_iota(jnp.int32, (LEN, LEN), 0) - lax.broadcasted_iota(
            jnp.int32, (LEN, LEN), 1
        )

        def body(h, carry):
            cols = cols_at(h, size)

            def turned(ref):
                v = ref[at(c), cols].astype(F32)
                swapped = jnp.where(even, -pltpu.roll(v, size - 1, 1), pltpu.roll(v, 1, 1))
                return v * r.cos[...] + swapped * r.sin[...]

            q = turned(r.a_query).astype(BF16)
            k = (turned(r.a_key) * size ** -0.5).astype(BF16)
            scores = lax.dot_general(q, k, (((1,), (1,)), ((), ())), preferred_element_type=F32)
            decay = jnp.exp(-r.rate[0, h] * jnp.maximum(distance, 0).astype(F32))
            scores = jnp.where(distance >= 0, scores * decay, 0.0).astype(BF16)
            kept = dot(scores, r.a_value[at(c), cols])
            kept = kept * lax.rsqrt(jnp.mean(kept * kept, axis=1, keepdims=True) + HEAD_EPS)
            r.kept[at(c), cols] = kept * r.ret_gain[:, cols]
            return carry

        lax.fori_loop(0, heads, body, 0)

    def gated(c):
        g = dot(r.normed[at(c), :], r.outgate[...]) * r.scale_outgate[...]
        g = g.astype(BF16).astype(F32)
        r.mixed[at(c), own] = (r.kept[at(c), :] * (g / (1.0 + jnp.exp(-g)))).astype(BF16)

    def spread_mix(offset):
        target = lax.rem(group.t + offset, ntp)
        there = cols_at(lax.rem(target, 2), half)
        place = pl.ds(pl.multiple_of(group.t * width, width), width)
        return remote(
            r.mix.at[:, there], r.mix_all.at[place], r.x_send.at[offset], r.x_recv.at[group.t],
            "tp", target,
        )

    def mix_arrived(offset):
        source = lax.rem(group.t + offset, ntp)
        place = pl.ds(pl.multiple_of(source * width, width), width)
        remote(
            r.mix.at[:, mine], r.mix_all.at[place], r.x_send.at[offset], r.x_recv.at[source],
            "tp", source,
        ).wait_recv()

    def swap(c):
        block = r.full_2.at[at(c), mine]
        return remote(block, block, r.h_send.at[c], r.h_recv.at[c], "tp", group.partner)

    def swapped(c):
        block = r.full_2.at[at(c), cols_at(1 - group.core, half)]
        remote(block, block, r.h_send.at[c], r.h_recv.at[c], "tp", group.partner).wait_recv()

    def second(c):
        tile = 512

        def body(n, carry):
            cols = cols_at(n, tile)
            there = pl.ds(pl.multiple_of(group.core * half + n * tile, tile), tile)
            total = dot(r.mixed[at(c), :], r.mix_all[:, cols]) * r.gains[3:4, there]
            r.full_2[at(c), there] = (r.full_1[at(c), there].astype(F32) + total).astype(BF16)
            return carry

        lax.fori_loop(0, half // tile, body, 0)

    def settle(i, c, res, out, place):
        value = res[at(c), own].astype(F32)
        value = value + 0.5 * reduces[i].total(c) * r.scale_down[...]
        out[at(c), place] = value.astype(BF16)

    gain_gather.relay(0)
    for c in chunks:
        stream.some(3)
        gathers[0].relay(c)
    gain_gather.complete(0)
    for c in chunks:
        stream.some(1)
        gathers[0].complete(c)
        norm(r.full_0, 0, c)
    need("gate")
    need("up")
    for c in chunks:
        gate_up(c)
        stream.some(1)
    need("down")
    for c in chunks:
        partial(c)
        reduces[0].start(c)
        stream.some(1)
    for c in chunks:
        reduces[0].cross(c)
        stream.some(2)
    for c in chunks:
        settle(0, c, r.full_0, r.full_1, own)
        gathers[1].start(c)
        stream.some(2)
    need("mix")
    for offset in range(1, ntp):
        spread_mix(offset).start()
    r.mix_all[pl.ds(pl.multiple_of(group.t * width, width), width), :] = r.mix[:, mine]
    for c in chunks:
        gathers[1].relay(c)
        stream.some(2)
    for c in chunks:
        gathers[1].complete(c)
        norm(r.full_1, 1, c)
        reduces[0].finish(c)
        stream.some(1)
    for table in table_loads:
        table.wait()
    for name in ("query", "key", "value"):
        need(name)
        project(name)
        stream.some(1)
    for c in chunks:
        retain(c)
        stream.some(1)
    need("outgate")
    for c in chunks:
        gated(c)
        gathers[2].start(c)
    for offset in range(1, ntp):
        mix_arrived(offset)
    gathers[2].relay(0)
    gathers[2].complete(0)
    second(0)
    swap(0).start()
    for c in chunks:
        swapped(c)
        norm(r.full_2, 2, c)
        if c == 0 and count > 1:
            gathers[2].relay(1)
        if c > 0:
            reduces[1].cross(c - 1)
        gate_up(c)
        if c + 1 < count:
            gathers[2].complete(c + 1)
            second(c + 1)
            swap(c + 1).start()
        partial(c)
        reduces[1].start(c)
        if c + 2 < count:
            gathers[2].relay(c + 2)
    reduces[1].cross(count - 1)
    for c in chunks:
        settle(1, c, r.full_2, r.out, pl.ds(0, width))
    for c in chunks:
        reduces[1].finish(c)
        swap(c).wait_send()
        for gather in gathers:
            gather.finish(c)
    for offset in range(1, ntp):
        spread_mix(offset).wait_send()
    gain_gather.finish(0)
    stream.finish()


def vmem():
    return pl.BlockSpec(memory_space=pltpu.VMEM)


def dma(*shape):
    return pltpu.SemaphoreType.DMA(shape)


def along_y_of(nfs, ntp):
    return ntp // 2 if nfs % (ntp // 2) == 0 else 1


def tables(length, width):
    freq = np.float32(1.0) / np.float32(10000.0) ** np.linspace(0.0, 1.0, width // 2, dtype=np.float32)
    angles = np.arange(length, dtype=np.float32)[:, None] * np.repeat(freq, 2)[None, :]
    return jnp.asarray(np.cos(angles)), jnp.asarray(np.sin(angles))


def per_device(
    nfs, ntp,
    tokens, gain_one, w_gate, w_up, w_down, scale_gate, scale_up, scale_down,
    gain_mix, w_query, w_key, w_value, w_outgate,
    scale_query, scale_key, scale_value, scale_outgate,
    ret_gain, decay_rate, w_mix, scale_mix, gain_two,
):
    ny, nx = along_y_of(nfs, ntp), ntp // 2
    rows, width = tokens.shape
    count = rows // LEN
    model = width * ntp
    weights = (w_gate, w_up, w_down, w_mix, w_query, w_key, w_value, w_outgate)
    cosines, sines = tables(LEN, width // decay_rate.shape[0])
    anywhere = pl.BlockSpec(memory_space=pl.ANY)
    inputs = {"w_" + name: (w, anywhere) for name, w in zip(WEIGHTS, weights)}
    inputs["tok"] = (tokens, anywhere)
    inputs["rate"] = (decay_rate[None], pl.BlockSpec(memory_space=pltpu.SMEM))
    inputs["cosines"], inputs["sines"] = (cosines, anywhere), (sines, anywhere)
    inputs["scale_gate"] = (scale_gate.reshape(-1, 128), vmem())
    inputs["scale_up"] = (scale_up.reshape(-1, 128), vmem())
    for name, value in (
        ("gain_one", gain_one), ("gain_mix", gain_mix), ("gain_two", gain_two),
        ("scale_down", scale_down), ("scale_query", scale_query), ("scale_key", scale_key),
        ("scale_value", scale_value), ("scale_outgate", scale_outgate),
        ("scale_mix", scale_mix), ("ret_gain", ret_gain),
    ):
        inputs[name] = (value[None], vmem())
    scratch = {}
    for name, w, dim in zip(WEIGHTS, weights, DIMS):
        grown = tuple(size * (nfs if axis == dim else 1) for axis, size in enumerate(w.shape))
        scratch[name] = pltpu.VMEM(grown, BF16)
    for i in range(3):
        shapes = [w.shape for w, stage in zip(weights, STAGES) if stage == i]
        scratch["stage_%d" % i] = pltpu.VMEM(tuple(max(sizes) for sizes in zip(*shapes)), F32)
    for name in ("full_0", "full_1", "full_2", "normed", "mixed", "part"):
        scratch[name] = pltpu.VMEM((rows, model), BF16)
    scratch["mix_all"] = pltpu.VMEM((model, model // 2), BF16)
    scratch["hidden"] = pltpu.VMEM((rows, w_gate.shape[1]), BF16)
    far = max(nx - 1, 1)
    scratch["pair"] = pltpu.VMEM((far, rows, width), BF16)
    scratch["one"] = pltpu.VMEM((2, nx, rows, width), BF16)
    scratch["two"] = pltpu.VMEM((2, far, rows, width), BF16)
    for name in ("a_query", "a_key", "a_value"):
        scratch[name] = pltpu.VMEM((rows, width), BF16)
    scratch["kept"] = pltpu.VMEM((rows, width), F32)
    scratch["cos"], scratch["sin"] = pltpu.VMEM(cosines.shape, F32), pltpu.VMEM(sines.shape, F32)
    scratch["s_gate"] = pltpu.VMEM((1, w_gate.shape[1]), F32)
    scratch["s_up"] = pltpu.VMEM((1, w_up.shape[1]), F32)
    scratch["gain_own"] = pltpu.VMEM((8, width), F32)
    scratch["gains"] = pltpu.VMEM((8, model), F32)
    total = 2 * len(WEIGHTS)
    scratch["load_sem"], scratch["tok_sem"] = dma(len(WEIGHTS)), dma()
    scratch["table_sem"] = dma(2)
    scratch["w_send"], scratch["w_recv"] = dma(ny + 1, nfs, total), dma(nfs, total)
    scratch["n_send"], scratch["n_fwd"], scratch["n_recv"] = dma(nx, 1), dma(nx, 1), dma(ntp, 1)
    scratch["g_send"], scratch["g_fwd"] = dma(3, nx, count), dma(3, nx, count)
    scratch["g_recv"] = dma(3, ntp, count)
    scratch["r_s1"], scratch["r_v1"] = dma(2, nx, count), dma(2, nx, count)
    scratch["r_s2"], scratch["r_v2"] = dma(2, far, count), dma(2, far, count)
    scratch["x_send"], scratch["x_recv"] = dma(ntp), dma(ntp)
    scratch["h_send"], scratch["h_recv"] = dma(count), dma(count)
    names = list(inputs) + ["out"] + list(scratch)
    return pl.pallas_call(
        functools.partial(layer_kernel, nfs, ntp, ny, names),
        out_shape=jax.ShapeDtypeStruct((rows, width), BF16),
        in_specs=[spec for _, spec in inputs.values()],
        out_specs=vmem(),
        scratch_shapes=list(scratch.values()),
        compiler_params=pltpu.CompilerParams(
            collective_id=0, has_side_effects=True, vmem_limit_bytes=67043328
        ),
        cost_estimate=pl.CostEstimate(flops=4 * 10**10, bytes_accessed=2**24, transcendentals=0),
        name="layer",
    )(*[value for value, _ in inputs.values()])


def solution(mesh):
    return jax.shard_map(
        functools.partial(per_device, mesh.shape["fs"], mesh.shape["tp"]),
        mesh=mesh,
        in_specs=(
            P("fs", "tp"), P("tp"), P("fs", "tp"), P("fs", "tp"), P("tp", "fs"),
            P("tp"), P("tp"), P("tp"), P("tp"),
            P("fs", "tp"), P("fs", "tp"), P("fs", "tp"), P("fs", "tp"),
            P("tp"), P("tp"), P("tp"), P("tp"), P("tp"), P("tp"),
            P("tp", "fs"), P("tp"), P("tp"),
        ),
        out_specs=P("fs", "tp"),
        check_vma=False,
    )
```

```python
import functools
from types import SimpleNamespace

import jax
import jax.numpy as jnp
import numpy as np
from jax import lax
from jax.experimental import pallas as pl
from jax.experimental.pallas import tpu as pltpu
from jax.sharding import PartitionSpec as P

LEN = 256
EPS = 1e-06
HEAD_EPS = 0.1
MESH = pl.DeviceIdType.MESH
BF16 = jnp.bfloat16
F32 = jnp.float32
WEIGHTS = ("gate", "up", "down", "mix", "query", "key", "value", "outgate")
DIMS = (0, 0, 1, 1, 0, 0, 0, 0)
STAGES = (0, 1, 2, 2, 0, 1, 0, 1)


def cols_at(index, width):
    return pl.ds(pl.multiple_of(index * width, width), width)


def remote(src, dst, send_sem, recv_sem, axis, target):
    return pltpu.make_async_remote_copy(
        src_ref=src,
        dst_ref=dst,
        send_sem=send_sem,
        recv_sem=recv_sem,
        device_id={axis: target},
        device_id_type=MESH,
    )


def dot(left, right):
    return jnp.dot(left, right, preferred_element_type=F32)


class TpGroup:
    def __init__(self, ntp):
        self.ntp, self.nx = ntp, ntp // 2
        self.t = lax.axis_index("tp")
        self.core, self.chip = lax.rem(self.t, 2), lax.div(self.t, 2)
        self.partner = self.chip * 2 + (1 - self.core)

    def along_x(self, offset, core):
        return lax.rem(self.chip + offset, self.nx) * 2 + core

    def greet(self, barrier):
        for offset in range(1, self.ntp):
            target = lax.rem(self.t + offset, self.ntp)
            pl.semaphore_signal(barrier, inc=1, device_id={"tp": target}, device_id_type=MESH)
        return self.ntp - 1


class TpGather:
    def __init__(self, group, out, sems, rows):
        self.group = group
        self.out, self.rows = out, rows
        self.sends, self.forwards, self.recvs = sems
        self.width = out.shape[1] // group.ntp

    def at(self, piece):
        return pl.ds(piece * self.rows, self.rows)

    def place(self, index, piece):
        return self.out.at[self.at(piece), cols_at(index, self.width)]

    def own_sends(self, piece):
        group = self.group
        copies = []
        for offset in range(group.nx - 1, -1, -1):
            target = group.along_x(offset, group.core) if offset else group.partner
            copies.append(
                remote(
                    self.place(group.t, piece), self.place(group.t, piece),
                    self.sends.at[offset, piece], self.recvs.at[group.t, piece], "tp", target,
                )
            )
        return copies

    def forward(self, offset, piece):
        group = self.group
        index = group.along_x(group.nx - offset, group.core)
        block = self.place(index, piece)
        return remote(
            block, block, self.forwards.at[offset, piece], self.recvs.at[index, piece],
            "tp", group.partner,
        )

    def arrived(self, index, piece):
        block = self.place(index, piece)
        remote(
            block, block, self.sends.at[0, piece], self.recvs.at[index, piece],
            "tp", self.group.partner,
        ).wait_recv()

    def start(self, piece):
        for copy in self.own_sends(piece):
            copy.start()

    def relay(self, piece):
        group = self.group
        for offset in range(1, group.nx):
            self.arrived(group.along_x(group.nx - offset, group.core), piece)
            self.forward(offset, piece).start()

    def complete(self, piece):
        group = self.group
        for offset in range(group.nx):
            self.arrived(group.along_x(offset, 1 - group.core), piece)

    def finish(self, piece):
        for copy in self.own_sends(piece):
            copy.wait_send()
        for offset in range(1, self.group.nx):
            self.forward(offset, piece).wait_send()


class TpReduce:
    def __init__(self, group, part, pair, one, two, sems, rows, width):
        self.group, self.part, self.pair, self.one, self.two = group, part, pair, one, two
        self.s1, self.v1, self.s2, self.v2 = sems
        self.rows, self.width = rows, width

    def at(self, piece):
        return pl.ds(piece * self.rows, self.rows)

    def block(self, offset, core):
        return cols_at(self.group.along_x(offset, core), self.width)

    def to_partner(self, offset, piece):
        return remote(
            self.part.at[self.at(piece), self.block(offset, 1 - self.group.core)],
            self.one.at[offset, self.at(piece)],
            self.s1.at[offset, piece], self.v1.at[offset, piece], "tp", self.group.partner,
        )

    def across(self, offset, piece):
        return remote(
            self.pair.at[offset - 1, self.at(piece)],
            self.two.at[offset - 1, self.at(piece)],
            self.s2.at[offset - 1, piece], self.v2.at[offset - 1, piece],
            "tp", self.group.along_x(offset, self.group.core),
        )

    def start(self, piece):
        for offset in range(self.group.nx - 1, -1, -1):
            self.to_partner(offset, piece).start()

    def cross(self, piece):
        at = self.at(piece)
        for offset in range(self.group.nx - 1, 0, -1):
            self.to_partner(offset, piece).wait_recv()
            mine = self.part[at, self.block(offset, self.group.core)].astype(F32)
            self.pair[offset - 1, at] = (mine + self.one[offset, at].astype(F32)).astype(BF16)
            self.across(offset, piece).start()

    def total(self, piece):
        at = self.at(piece)
        self.to_partner(0, piece).wait_recv()
        value = self.part[at, self.block(0, self.group.core)].astype(F32)
        value = value + self.one[0, at].astype(F32)
        for offset in range(1, self.group.nx):
            self.across(offset, piece).wait_recv()
            value = value + self.two[offset - 1, at].astype(F32)
        return value

    def finish(self, piece):
        for offset in range(self.group.nx):
            self.to_partner(offset, piece).wait_send()
        for offset in range(1, self.group.nx):
            self.across(offset, piece).wait_send()


class FsStream:
    def __init__(self, nfs, ny, pieces, sends, recvs):
        self.ny, self.nz = ny, nfs // ny
        self.f = lax.axis_index("fs")
        self.z, self.y = lax.div(self.f, ny), lax.rem(self.f, ny)
        self.pieces = pieces
        self.sends, self.recvs = sends, recvs
        self.events, self.done = self.schedule(), 0

    def whole_z(self, p):
        return self.pieces[p].along_z

    def place(self, p, index):
        piece = self.pieces[p]
        if piece.dim == 0:
            start = pl.multiple_of(index * piece.rows + piece.start, 16)
            return piece.buf.at[pl.ds(start, piece.size)]
        return piece.buf.at[pl.ds(piece.start, piece.size), cols_at(index, piece.cols)]

    def move(self, p, kind, index, target):
        block = self.place(p, index)
        return remote(
            block, block, self.sends.at[kind, index, p], self.recvs.at[index, p], "fs", target
        )

    def arrived(self, p, index):
        self.move(p, 0, index, self.f).wait_recv()

    def move_z(self, p, step, index, act):
        inside = (self.z < self.nz - 1) if step > 0 else (self.z > 0)

        @pl.when(inside)
        def _():
            act(self.move(p, 0 if step > 0 else 1, index, self.f + step * self.ny))

    def move_y(self, p, index, act):
        for offset in range(1, self.ny):
            target = self.z * self.ny + lax.rem(self.y + offset, self.ny)
            act(self.move(p, 1 + offset, index, target))

    def others(self, zs):
        return [zs * self.ny + lax.rem(self.y + offset, self.ny) for offset in range(1, self.ny)]

    def own(self, p, act, wait):
        self.move_y(p, self.f, act)
        for step in (1, -1):
            self.move_z(p, step, self.f, act)

    def side(self, p, act, wait):
        for index in self.others(self.z):
            if wait:
                self.arrived(p, index)
            for step in (1, -1):
                self.move_z(p, step, index, act)

    def relay(self, distance, p, act, wait):
        for step in (1, -1):
            zs = self.z - step * distance

            @pl.when(jnp.logical_and(zs >= 0, zs < self.nz))
            def _():
                same = zs * self.ny + self.y
                for index in [same] + (self.others(zs) if self.whole_z(p) else []):
                    if wait:
                        self.arrived(p, index)
                    self.move_z(p, step, index, act)
                    if not self.whole_z(p):
                        self.move_y(p, index, act)

    def schedule(self):
        events = []
        for p in range(len(self.pieces)):
            late = self.whole_z(p)
            events.append((p - 1.3 + 0.5 * late, p, functools.partial(self.own, p)))
            if late:
                events.append((p + 1.2, p, functools.partial(self.side, p)))
            for distance in range(1, self.nz):
                when = p + 0.75 * distance + (1.55 if late else -0.4)
                events.append((when, p, functools.partial(self.relay, distance, p)))
        events.sort(key=lambda event: event[:2])
        return [event[1:] for event in events]

    def some(self, count):
        for _, event in self.events[self.done : self.done + count]:
            event(lambda copy: copy.start(), True)
        self.done = min(self.done + count, len(self.events))

    def need(self, p):
        last = max(i for i, (piece, _) in enumerate(self.events) if piece == p)
        self.some(max(0, last + 1 - self.done))
        if not self.whole_z(p):
            for zs in range(self.nz):
                for index in self.others(zs):
                    self.arrived(p, index)

    def finish(self):
        for _, event in self.events:
            event(lambda copy: copy.wait_send(), False)

    def greet(self, barrier):
        ny, z, f = self.ny, self.z, self.f
        for index in self.others(z):
            pl.semaphore_signal(barrier, inc=1, device_id={"fs": index}, device_id_type=MESH)

        @pl.when(z > 0)
        def _():
            pl.semaphore_signal(barrier, inc=1, device_id={"fs": f - ny}, device_id_type=MESH)

        @pl.when(z < self.nz - 1)
        def _():
            pl.semaphore_signal(barrier, inc=1, device_id={"fs": f + ny}, device_id_type=MESH)

        ends = (z > 0).astype(jnp.int32) + (z < self.nz - 1).astype(jnp.int32)
        return ends + (ny - 1)


def layer_kernel(nfs, ntp, ny, names, *refs):
    r = SimpleNamespace(**dict(zip(names, refs)))
    rows, width = r.out.shape
    model = width * ntp
    half = model // 2
    count = rows // LEN
    chunks = range(count)
    group = TpGroup(ntp)
    shards = [getattr(r, "w_" + name) for name in WEIGHTS]
    wholes = [getattr(r, name) for name in WEIGHTS]
    pieces, held = [], {name: [] for name in WEIGHTS}
    for i, name in enumerate(WEIGHTS):
        height, cols = shards[i].shape
        along_z = max(16, height * 3 // 16 // 16 * 16)
        for late, start, size in ((True, 0, along_z), (False, along_z, height - along_z)):
            held[name].append(len(pieces))
            pieces.append(
                SimpleNamespace(
                    buf=wholes[i], dim=DIMS[i], rows=height, cols=cols,
                    start=start, size=size, along_z=late,
                )
            )
    stream = FsStream(nfs, ny, pieces, r.w_send, r.w_recv)

    def need(name):
        for p in held[name]:
            stream.need(p)

    def at(c):
        return pl.ds(c * LEN, LEN)

    own = cols_at(group.t, width)
    mine = cols_at(group.core, half)
    stages = [r.stage_0, r.stage_1, r.stage_2]

    def load(i):
        height, cols = shards[i].shape
        stage = stages[STAGES[i]].at[pl.ds(0, height), pl.ds(0, cols)]
        return pltpu.make_async_copy(shards[i], stage, r.load_sem.at[i])

    def cast(i):
        load(i).wait()
        height, cols = shards[i].shape
        value = stages[STAGES[i]][0:height, 0:cols].astype(BF16)
        if DIMS[i] == 0:
            wholes[i][pl.ds(pl.multiple_of(stream.f * height, height), height), :] = value
        else:
            wholes[i][:, cols_at(stream.f, cols)] = value

    barrier = pltpu.get_barrier_semaphore()
    greeted = group.greet(barrier) + stream.greet(barrier)
    tok_load = pltpu.make_async_copy(r.tok, r.full_0.at[:, own], r.tok_sem)
    table_loads = [
        pltpu.make_async_copy(src, dst, r.table_sem.at[i])
        for i, (src, dst) in enumerate(((r.cosines, r.cos), (r.sines, r.sin)))
    ]
    load(0).start()
    tok_load.start()
    load(1).start()
    load(2).start()
    for table in table_loads:
        table.start()
    r.gain_own[...] = jnp.zeros(r.gain_own.shape, F32)
    for row, ref in enumerate((r.gain_one, r.gain_mix, r.gain_two, r.scale_mix)):
        r.gain_own[row : row + 1, :] = ref[...]
    r.gains[:, own] = r.gain_own[...]
    for src, dst in ((r.scale_gate, r.s_gate), (r.scale_up, r.s_up)):
        for row in range(src.shape[0]):
            dst[:, row * 128 : (row + 1) * 128] = src[row : row + 1, :]
    cast(0)
    pl.semaphore_wait(barrier, greeted)

    gain_gather = TpGather(group, r.gains, (r.n_send, r.n_fwd, r.n_recv), 8)
    gathers = [
        TpGather(group, full, (r.g_send.at[i], r.g_fwd.at[i], r.g_recv.at[i]), LEN)
        for i, full in enumerate((r.full_0, r.full_1, r.mixed))
    ]
    reduces = [
        TpReduce(
            group, r.part, r.pair, r.one.at[i], r.two.at[i],
            (r.r_s1.at[i], r.r_v1.at[i], r.r_s2.at[i], r.r_v2.at[i]), LEN, width,
        )
        for i in range(2)
    ]
    stream.some(2)
    gain_gather.start(0)
    tok_load.wait()
    for c in chunks:
        gathers[0].start(c)
    cast(1)
    load(4).start()
    load(5).start()
    cast(2)
    load(3).start()
    stream.some(2)
    cast(3)
    cast(4)
    load(6).start()
    cast(5)
    load(7).start()
    cast(6)
    cast(7)

    def norm(full, row, c):
        gain = r.gains[row : row + 1, :]
        step = 32

        def body(i, carry):
            some = pl.ds(pl.multiple_of(c * LEN + i * step, step), step)
            v = full[some, :].astype(F32)
            mean = jnp.mean(v * v, axis=1, keepdims=True)
            r.normed[some, :] = (v * lax.rsqrt(mean + EPS) * gain).astype(BF16)
            return carry

        lax.fori_loop(0, LEN // step, body, 0, unroll=4)

    def gate_up(c):
        x = r.normed[at(c), :]
        g = dot(x, r.gate[...]) * r.s_gate[...]
        u = dot(x, r.up[...]) * r.s_up[...]
        r.hidden[at(c), :] = (g / (1.0 + jnp.exp(-g)) * u).astype(BF16)

    def partial(c):
        def body(n, carry):
            cols = cols_at(n, half)
            r.part[at(c), cols] = dot(r.hidden[at(c), :], r.down[:, cols]).astype(BF16)
            return carry

        lax.fori_loop(0, 2, body, 0)

    def project(name):
        weight, scale, out = getattr(r, name), getattr(r, "scale_" + name), getattr(r, "a_" + name)

        def body(c, carry):
            some = pl.ds(pl.multiple_of(c * LEN, LEN), LEN)
            out[some, :] = (dot(r.normed[some, :], weight[...]) * scale[...]).astype(BF16)
            return carry

        lax.fori_loop(0, count, body, 0)

    heads = r.rate.shape[1]
    size = width // heads

    def retain(c):
        even = lax.rem(lax.broadcasted_iota(jnp.int32, (LEN, size), 1), 2) == 0
        distance = lax.broadcasted_iota(jnp.int32, (LEN, LEN), 0) - lax.broadcasted_iota(
            jnp.int32, (LEN, LEN), 1
        )

        def body(h, carry):
            cols = cols_at(h, size)

            def turned(ref):
                v = ref[at(c), cols].astype(F32)
                swapped = jnp.where(even, -pltpu.roll(v, size - 1, 1), pltpu.roll(v, 1, 1))
                return v * r.cos[...] + swapped * r.sin[...]

            q = turned(r.a_query).astype(BF16)
            k = (turned(r.a_key) * size ** -0.5).astype(BF16)
            scores = lax.dot_general(q, k, (((1,), (1,)), ((), ())), preferred_element_type=F32)
            decay = jnp.exp(-r.rate[0, h] * jnp.maximum(distance, 0).astype(F32))
            scores = jnp.where(distance >= 0, scores * decay, 0.0).astype(BF16)
            kept = dot(scores, r.a_value[at(c), cols])
            kept = kept * lax.rsqrt(jnp.mean(kept * kept, axis=1, keepdims=True) + HEAD_EPS)
            r.kept[at(c), cols] = kept * r.ret_gain[:, cols]
            return carry

        lax.fori_loop(0, heads, body, 0)

    def gated(c):
        g = dot(r.normed[at(c), :], r.outgate[...]) * r.scale_outgate[...]
        g = g.astype(BF16).astype(F32)
        r.mixed[at(c), own] = (r.kept[at(c), :] * (g / (1.0 + jnp.exp(-g)))).astype(BF16)

    def spread_mix(offset):
        target = lax.rem(group.t + offset, ntp)
        there = cols_at(lax.rem(target, 2), half)
        place = pl.ds(pl.multiple_of(group.t * width, width), width)
        return remote(
            r.mix.at[:, there], r.mix_all.at[place], r.x_send.at[offset], r.x_recv.at[group.t],
            "tp", target,
        )

    def mix_arrived(offset):
        source = lax.rem(group.t + offset, ntp)
        place = pl.ds(pl.multiple_of(source * width, width), width)
        remote(
            r.mix.at[:, mine], r.mix_all.at[place], r.x_send.at[offset], r.x_recv.at[source],
            "tp", source,
        ).wait_recv()

    def swap(c):
        block = r.full_2.at[at(c), mine]
        return remote(block, block, r.h_send.at[c], r.h_recv.at[c], "tp", group.partner)

    def swapped(c):
        block = r.full_2.at[at(c), cols_at(1 - group.core, half)]
        remote(block, block, r.h_send.at[c], r.h_recv.at[c], "tp", group.partner).wait_recv()

    def second(c):
        total = dot(r.mixed[at(c), :], r.mix_all[...]) * r.gains[3:4, mine]
        r.full_2[at(c), mine] = (r.full_1[at(c), mine].astype(F32) + total).astype(BF16)

    def settle(i, c, res, out, place):
        value = res[at(c), own].astype(F32)
        value = value + 0.5 * reduces[i].total(c) * r.scale_down[...]
        out[at(c), place] = value.astype(BF16)

    gain_gather.relay(0)
    for c in chunks:
        stream.some(3)
        gathers[0].relay(c)
    gain_gather.complete(0)
    for c in chunks:
        stream.some(1)
        gathers[0].complete(c)
        norm(r.full_0, 0, c)
    need("gate")
    need("up")
    for c in chunks:
        gate_up(c)
        stream.some(1)
    need("down")
    for c in chunks:
        partial(c)
        reduces[0].start(c)
        stream.some(1)
    for c in chunks:
        reduces[0].cross(c)
        stream.some(2)
    for c in chunks:
        settle(0, c, r.full_0, r.full_1, own)
        gathers[1].start(c)
        stream.some(2)
    need("mix")
    for offset in range(1, ntp):
        spread_mix(offset).start()
    r.mix_all[pl.ds(pl.multiple_of(group.t * width, width), width), :] = r.mix[:, mine]
    for c in chunks:
        gathers[1].relay(c)
        stream.some(2)
    for c in chunks:
        gathers[1].complete(c)
        norm(r.full_1, 1, c)
        reduces[0].finish(c)
        stream.some(1)
    for table in table_loads:
        table.wait()
    for name in ("query", "key", "value"):
        need(name)
        project(name)
        stream.some(1)
    for c in chunks:
        retain(c)
        stream.some(1)
    need("outgate")
    for c in chunks:
        gated(c)
        gathers[2].start(c)
    for offset in range(1, ntp):
        mix_arrived(offset)
    gathers[2].relay(0)
    gathers[2].complete(0)
    second(0)
    swap(0).start()
    for c in chunks:
        swapped(c)
        norm(r.full_2, 2, c)
        if c == 0 and count > 1:
            gathers[2].relay(1)
        if c > 0:
            reduces[1].cross(c - 1)
        gate_up(c)
        if c + 1 < count:
            gathers[2].complete(c + 1)
            second(c + 1)
            swap(c + 1).start()
        partial(c)
        reduces[1].start(c)
        if c + 2 < count:
            gathers[2].relay(c + 2)
    reduces[1].cross(count - 1)
    for c in chunks:
        settle(1, c, r.full_2, r.out, pl.ds(0, width))
    for c in chunks:
        reduces[1].finish(c)
        swap(c).wait_send()
        for gather in gathers:
            gather.finish(c)
    for offset in range(1, ntp):
        spread_mix(offset).wait_send()
    gain_gather.finish(0)
    stream.finish()


def vmem():
    return pl.BlockSpec(memory_space=pltpu.VMEM)


def dma(*shape):
    return pltpu.SemaphoreType.DMA(shape)


def along_y_of(nfs, ntp):
    return ntp // 2 if nfs % (ntp // 2) == 0 else 1


def tables(length, width):
    freq = np.float32(1.0) / np.float32(10000.0) ** np.linspace(0.0, 1.0, width // 2, dtype=np.float32)
    angles = np.arange(length, dtype=np.float32)[:, None] * np.repeat(freq, 2)[None, :]
    return jnp.asarray(np.cos(angles)), jnp.asarray(np.sin(angles))


def per_device(
    nfs, ntp,
    tokens, gain_one, w_gate, w_up, w_down, scale_gate, scale_up, scale_down,
    gain_mix, w_query, w_key, w_value, w_outgate,
    scale_query, scale_key, scale_value, scale_outgate,
    ret_gain, decay_rate, w_mix, scale_mix, gain_two,
):
    ny, nx = along_y_of(nfs, ntp), ntp // 2
    rows, width = tokens.shape
    count = rows // LEN
    model = width * ntp
    weights = (w_gate, w_up, w_down, w_mix, w_query, w_key, w_value, w_outgate)
    cosines, sines = tables(LEN, width // decay_rate.shape[0])
    anywhere = pl.BlockSpec(memory_space=pl.ANY)
    inputs = {"w_" + name: (w, anywhere) for name, w in zip(WEIGHTS, weights)}
    inputs["tok"] = (tokens, anywhere)
    inputs["rate"] = (decay_rate[None], pl.BlockSpec(memory_space=pltpu.SMEM))
    inputs["cosines"], inputs["sines"] = (cosines, anywhere), (sines, anywhere)
    inputs["scale_gate"] = (scale_gate.reshape(-1, 128), vmem())
    inputs["scale_up"] = (scale_up.reshape(-1, 128), vmem())
    for name, value in (
        ("gain_one", gain_one), ("gain_mix", gain_mix), ("gain_two", gain_two),
        ("scale_down", scale_down), ("scale_query", scale_query), ("scale_key", scale_key),
        ("scale_value", scale_value), ("scale_outgate", scale_outgate),
        ("scale_mix", scale_mix), ("ret_gain", ret_gain),
    ):
        inputs[name] = (value[None], vmem())
    scratch = {}
    for name, w, dim in zip(WEIGHTS, weights, DIMS):
        grown = tuple(size * (nfs if axis == dim else 1) for axis, size in enumerate(w.shape))
        scratch[name] = pltpu.VMEM(grown, BF16)
    for i in range(3):
        shapes = [w.shape for w, stage in zip(weights, STAGES) if stage == i]
        scratch["stage_%d" % i] = pltpu.VMEM(tuple(max(sizes) for sizes in zip(*shapes)), F32)
    for name in ("full_0", "full_1", "full_2", "normed", "mixed", "part"):
        scratch[name] = pltpu.VMEM((rows, model), BF16)
    scratch["mix_all"] = pltpu.VMEM((model, model // 2), BF16)
    scratch["hidden"] = pltpu.VMEM((rows, w_gate.shape[1]), BF16)
    far = max(nx - 1, 1)
    scratch["pair"] = pltpu.VMEM((far, rows, width), BF16)
    scratch["one"] = pltpu.VMEM((2, nx, rows, width), BF16)
    scratch["two"] = pltpu.VMEM((2, far, rows, width), BF16)
    for name in ("a_query", "a_key", "a_value"):
        scratch[name] = pltpu.VMEM((rows, width), BF16)
    scratch["kept"] = pltpu.VMEM((rows, width), F32)
    scratch["cos"], scratch["sin"] = pltpu.VMEM(cosines.shape, F32), pltpu.VMEM(sines.shape, F32)
    scratch["s_gate"] = pltpu.VMEM((1, w_gate.shape[1]), F32)
    scratch["s_up"] = pltpu.VMEM((1, w_up.shape[1]), F32)
    scratch["gain_own"] = pltpu.VMEM((8, width), F32)
    scratch["gains"] = pltpu.VMEM((8, model), F32)
    total = 2 * len(WEIGHTS)
    scratch["load_sem"], scratch["tok_sem"] = dma(len(WEIGHTS)), dma()
    scratch["table_sem"] = dma(2)
    scratch["w_send"], scratch["w_recv"] = dma(ny + 1, nfs, total), dma(nfs, total)
    scratch["n_send"], scratch["n_fwd"], scratch["n_recv"] = dma(nx, 1), dma(nx, 1), dma(ntp, 1)
    scratch["g_send"], scratch["g_fwd"] = dma(3, nx, count), dma(3, nx, count)
    scratch["g_recv"] = dma(3, ntp, count)
    scratch["r_s1"], scratch["r_v1"] = dma(2, nx, count), dma(2, nx, count)
    scratch["r_s2"], scratch["r_v2"] = dma(2, far, count), dma(2, far, count)
    scratch["x_send"], scratch["x_recv"] = dma(ntp), dma(ntp)
    scratch["h_send"], scratch["h_recv"] = dma(count), dma(count)
    names = list(inputs) + ["out"] + list(scratch)
    return pl.pallas_call(
        functools.partial(layer_kernel, nfs, ntp, ny, names),
        out_shape=jax.ShapeDtypeStruct((rows, width), BF16),
        in_specs=[spec for _, spec in inputs.values()],
        out_specs=vmem(),
        scratch_shapes=list(scratch.values()),
        compiler_params=pltpu.CompilerParams(
            collective_id=0, has_side_effects=True, vmem_limit_bytes=67043328
        ),
        cost_estimate=pl.CostEstimate(flops=4 * 10**10, bytes_accessed=2**24, transcendentals=0),
        name="layer",
    )(*[value for value, _ in inputs.values()])


def solution(mesh):
    return jax.shard_map(
        functools.partial(per_device, mesh.shape["fs"], mesh.shape["tp"]),
        mesh=mesh,
        in_specs=(
            P("fs", "tp"), P("tp"), P("fs", "tp"), P("fs", "tp"), P("tp", "fs"),
            P("tp"), P("tp"), P("tp"), P("tp"),
            P("fs", "tp"), P("fs", "tp"), P("fs", "tp"), P("fs", "tp"),
            P("tp"), P("tp"), P("tp"), P("tp"), P("tp"), P("tp"),
            P("tp", "fs"), P("tp"), P("tp"),
        ),
        out_specs=P("fs", "tp"),
        check_vma=False,
    )
```
